128 devices in a mesh: sp: 64 (over z, y, x), tp: 2 (over core).
Axes of the slice: x: 4, y: 4, z: 4, core: 2. Of those that a mesh axis runs over, the one named last changes fastest.
Arguments:
- resid: bfloat16 [16384, 2048], P(('sp', 'tp')), may hold values from -6 to 6
- value_in: bfloat16 [16384, 1536], P('sp', 'tp'), may hold values from -6 to 6
- gate_in: bfloat16 [16384, 1536], P('sp', 'tp'), may hold values from -8 to 8
- conv_weight: float32 [31, 1536], P(None, 'tp'), may hold values from -2.5 to 2.5
- norm_gain: float32 [1536], P('tp'), may hold values from 0.1 to 1.9
- out_weight: bfloat16 [1536, 2048], replicated, may hold values from -0.15625 to 0.15625
- ffn_gain: float32 [2048], replicated, may hold values from 0.1 to 1.9
- expert_ids: int32 [16384, 2], P(('sp', 'tp')), may hold values from 0 to 127, all different within a row; in each aligned block of 128 rows (0 to 127, 128 to 255, ...) at most 4 rows name the same one
- expert_mix: float32 [16384, 2], P(('sp', 'tp')), may hold values from 0.1 to 1
- w_gate: bfloat16 [128, 2048, 1024], P(('sp', 'tp')), may hold values from -0.125 to 0.125
- w_up: bfloat16 [128, 2048, 1024], P(('sp', 'tp')), may hold values from -0.125 to 0.125
- w_down: bfloat16 [128, 1024, 2048], P(('sp', 'tp')), may hold values from -0.1875 to 0.1875
Outputs:
- layer_out: bfloat16 [16384, 2048], P(('sp', 'tp'))
The draws below stay inside these ranges and needn't reach their ends.
Inputs may be any that keep to these rules, and one draw needn't show every extreme that they name: `expert_ids`: each row names 2 different experts; within each aligned block of 128 rows no expert is named by more than 4 rows, a bound that some block reaches.
All inputs are finite; a program needn't handle non-finite values.
Results may differ from the reference program's by a relative error of at most 0.012.
Values may be sent and summed in bfloat16 or wider, within the bound.
A program may use at most 128 MiB of HBM per device.

```python
import math
import jax
import jax.numpy as jnp
import numpy as np
from jax import lax

D = 2048
MIX = 1536
FF = 1024
CONV = 31
TOPK = 2
TOKENS = 16384
ROWS = 128
EXPERTS = 128
CAP = 4


def draw_conv_weight(key, part):
    first = jax.random.fold_in(key, 0)
    place = jnp.arange(MIX, dtype=jnp.float32) / max(MIX - 1, 1)
    scale = jnp.exp(jnp.log(4.0) * place)
    taps = jax.random.normal(first, (CONV, MIX), jnp.float32) * CONV ** (-0.5) * scale
    return jnp.clip(taps, -2.5, 2.5)


def steps_of(rng, extent, cuts, least, top_value):
    level = 1.0
    for dim, shards_of in cuts:
        steps = jax.random.uniform(jax.random.fold_in(jax.random.fold_in(rng, 6), dim), (shards_of,), jnp.float32, least / len(cuts), top_value / len(cuts))
        level = level * jnp.repeat(jnp.exp(steps), extent[dim] // shards_of).reshape((-1,) + (1,) * (len(extent) - 1 - dim))
    return level


def shared_out(stream_key, own, number, rows, number_of, top, bound, slope):
    ranking = jax.random.permutation(stream_key, number_of)
    packed, ordinary = portions_of(number_of, rows * top, bound, slope, True), portions_of(number_of, rows * top, bound, slope, False)
    places = jnp.arange(number_of)

    def named(tallies, turn):
        used = int((tallies > 0).sum())
        fixed = max(1, used // 4)
        passed = fixed + (places - fixed + turn * (used - fixed)) % max(1, number_of - fixed)
        return jnp.zeros((number_of,), jnp.int32).at[ranking[jnp.where(places < fixed, places, passed)]].set(jnp.asarray(tallies, jnp.int32))

    tallies = jnp.where(number % 4 == 0, named(packed, number // 4), named(ordinary, number - number // 4 - 1))
    mixed = jax.random.permutation(jax.random.fold_in(own, 3), number_of)
    source_of, sink = mixed[0:number_of // 2 * 2:2], mixed[1:number_of // 2 * 2:2]
    room = jnp.minimum(tallies[source_of] - 1, bound - tallies[sink]) // 2
    room = jnp.where((source_of == ranking[0]) | (sink == ranking[0]) | (tallies[sink] == 0), 0, jnp.maximum(room, 0))
    passed = jax.random.randint(jax.random.fold_in(own, 4), (number_of // 2,), 0, 1 << 20) % (room + 1)
    tallies = tallies.at[source_of].add(-passed).at[sink].add(passed)
    members = jnp.searchsorted(jnp.cumsum(tallies), jnp.arange(rows * top), side="right").astype(jnp.int32)
    listing = members.reshape(top, rows).T
    listing = listing[jax.random.permutation(jax.random.fold_in(own, 1), rows)]
    turn = jax.random.randint(jax.random.fold_in(own, 2), (rows, 1), 0, top)
    return jnp.take_along_axis(listing, (jnp.arange(top)[None, :] + turn) % top, axis=1)


def portions_of(amount, total, bound, lean, full):
    weights = [(1 << 20) // math.isqrt(grade ** lean) + 1 for grade in range(1, amount + 1)]
    largest = bound if full else min(bound, max(-(-total // amount), total * weights[0] // sum(weights)))
    least = 1 if total - largest >= amount - 1 else 0
    counts, surplus = [largest] + [least] * (amount - 1), total - largest - least * (amount - 1)
    while surplus > 0:
        candidates = [i for i in range(1, amount) if counts[i] < largest] or [i for i in range(1, amount) if counts[i] < bound]
        pool, left = sum([weights[i] for i in candidates]), surplus
        for i in candidates:
            more = min(bound - counts[i], max(1, left * weights[i] // pool), surplus)
            counts[i] = counts[i] + more
            surplus = surplus - more
    return np.array(counts)


def centred(own_key, dims, spread, limit, cuts=(), held_as=jnp.bfloat16):
    gain = steps_of(own_key, dims, cuts, -0.22, 0.18) if cuts else 1.0
    drawn = jax.random.normal(own_key, dims, jnp.float32) * spread * gain
    return jnp.minimum(jnp.maximum(drawn, -limit), limit).astype(held_as)


def setup_inputs(seed: int = 0) -> dict:
    streams_of = jax.random.split(jax.random.key(seed), 13)
    resid = centred(streams_of[0], (TOKENS, D), 1.0, 6.0, ((0, 128),))
    value_in = centred(streams_of[1], (TOKENS, MIX), 1.0, 6.0, ((0, 64), (1, 2)))
    gate_in = centred(streams_of[2], (TOKENS, MIX), 1.5, 8.0, ((0, 64), (1, 2)))
    conv_weight = draw_conv_weight(jax.random.fold_in(streams_of[12], 71), 0)
    norm_gain = jnp.clip(1.0 + 0.18 * jax.random.normal(streams_of[4], (MIX,), jnp.float32), 0.1, 1.9)
    out_weight = centred(streams_of[5], (MIX, D), MIX ** -0.5, 0.15625)
    ffn_gain = jnp.clip(1.0 + 0.18 * jax.random.normal(streams_of[6], (D,), jnp.float32), 0.1, 1.9)
    expert_ids_keys = jax.random.split(jax.random.fold_in(streams_of[7], 1), TOKENS // ROWS)
    expert_ids_turns = jax.random.permutation(jax.random.fold_in(streams_of[7], 3), TOKENS // ROWS)
    expert_ids = jax.vmap(lambda own, number: shared_out(jax.random.fold_in(streams_of[7], 2), own, number, ROWS, EXPERTS, TOPK, CAP, 2))(expert_ids_keys, expert_ids_turns).reshape((TOKENS, TOPK))
    expert_mix = jnp.clip(0.1 + 0.9 * jax.random.uniform(streams_of[8], (TOKENS, TOPK), jnp.float32) ** steps_of(streams_of[8], (TOKENS, TOPK), ((0, 128),), -0.2, 0.2), 0.1, 1.0)
    w_gate = centred(streams_of[9], (EXPERTS, D, FF), D ** -0.5, 0.125, ((0, 128),))
    w_up = centred(streams_of[10], (EXPERTS, D, FF), D ** -0.5, 0.125, ((0, 128),))
    w_down = centred(streams_of[11], (EXPERTS, FF, D), FF ** -0.5, 0.1875, ((0, 128),))
    return {"resid": resid, "value_in": value_in, "gate_in": gate_in, "conv_weight": conv_weight, "norm_gain": norm_gain, "out_weight": out_weight, "ffn_gain": ffn_gain, "expert_ids": expert_ids, "expert_mix": expert_mix, "w_gate": w_gate, "w_up": w_up, "w_down": w_down}


def reference(resid, value_in, gate_in, conv_weight, norm_gain, out_weight, ffn_gain, expert_ids, expert_mix, w_gate, w_up, w_down):
    glu = (value_in.astype(jnp.float32) * jax.nn.sigmoid(gate_in.astype(jnp.float32))).astype(jnp.bfloat16)
    reach = CONV // 2
    padded = jnp.pad(glu.astype(jnp.float32), ((reach, reach), (0, 0)))
    conv = jnp.zeros((TOKENS, MIX), jnp.float32)
    for tap in range(CONV):
        conv = conv + padded[tap:tap + TOKENS] * conv_weight[tap]
    mean = lax.optimization_barrier(jnp.mean(conv, axis=1, keepdims=True))
    msq = lax.optimization_barrier(jnp.mean(conv * conv, axis=1, keepdims=True))
    var = msq - mean * mean
    mixed = jax.nn.silu((conv - mean) * lax.rsqrt(var + 1e-05) * norm_gain).astype(jnp.bfloat16)
    proj = jnp.dot(mixed, out_weight, preferred_element_type=jnp.float32)
    stream = (resid.astype(jnp.float32) + proj).astype(jnp.bfloat16)
    wide = stream.astype(jnp.float32)
    normed = (wide * lax.rsqrt(lax.optimization_barrier(jnp.mean(wide * wide, axis=1, keepdims=True)) + 1e-06) * ffn_gain).astype(jnp.bfloat16)
    blocks = TOKENS // ROWS
    chosen = expert_ids.reshape(blocks, ROWS * TOPK)
    onehot = (chosen[:, :, None] == jnp.arange(EXPERTS, dtype=jnp.int32)[None, None, :]).astype(jnp.int32)
    rank = lax.optimization_barrier(jnp.sum(jnp.cumsum(onehot, axis=1) * onehot, axis=2)) - 1
    slot = jnp.arange(blocks, dtype=jnp.int32)[:, None] * CAP + rank
    token = jnp.arange(blocks, dtype=jnp.int32)[:, None] * ROWS + jnp.arange(ROWS * TOPK, dtype=jnp.int32)[None, :] // TOPK
    table = jnp.full((EXPERTS, blocks * CAP), TOKENS, jnp.int32)
    table = table.at[chosen.reshape(-1), slot.reshape(-1)].set(token.reshape(-1).astype(jnp.int32))
    source = jnp.concatenate([normed, jnp.zeros((1, D), jnp.bfloat16)], axis=0)

    def run(args):
        index, gate_w, up_w, down_w = args
        rows = jnp.take(source, index, axis=0)
        gate = jnp.dot(rows, gate_w, preferred_element_type=jnp.float32)
        up = jnp.dot(rows, up_w, preferred_element_type=jnp.float32)
        hidden = (jax.nn.silu(gate) * up).astype(jnp.bfloat16)
        return jnp.dot(hidden, down_w, preferred_element_type=jnp.float32).astype(jnp.bfloat16)
    results = lax.map(run, (table, w_gate, w_up, w_down))
    picked = results[chosen.reshape(-1), slot.reshape(-1)].astype(jnp.float32).reshape(TOKENS, TOPK, D)
    total = stream.astype(jnp.float32) + lax.optimization_barrier(jnp.sum(picked * expert_mix[:, :, None], axis=1))
    return total.astype(jnp.bfloat16)
```

```python
import functools

import jax
import jax.numpy as jnp
from jax import lax
from jax.experimental import pallas as pl
from jax.experimental.pallas import tpu as pltpu
from jax.sharding import PartitionSpec as P

MESH = pl.DeviceIdType.MESH
BF = jnp.bfloat16
F32 = jnp.float32
CAP = 4
N = 128
HALF = 64
TILE = 512


def padded_2(block, sides, width):
    for axis, dim in sides:
        count = lax.axis_size(axis)
        forward = [(i, i + 1) for i in range(count - 1)]
        backward = [(target, source) for source, target in forward]
        low = lax.ppermute(
            lax.slice_in_dim(block, block.shape[dim] - width, None, axis=dim), axis, forward
        )
        high = lax.ppermute(lax.slice_in_dim(block, 0, width, axis=dim), axis, backward)
        block = jnp.concatenate([low, block, high], axis=dim)
    return block


def offsets(i):
    a, b, c = i % 4, (i // 4) % 4, (i // 16) % 4
    return a, (a + b) % 4, (a + b + c) % 4, i // 64


def device_at(i, sign):
    sp, tp = lax.axis_index("sp"), lax.axis_index("tp")
    dz, dy, dx, dc = offsets(i)
    z, y, x = sp // 16, (sp // 4) % 4, sp % 4
    z, y, x = (z + 4 + sign * dz) % 4, (y + 4 + sign * dy) % 4, (x + 4 + sign * dx) % 4
    return (z * 4 + y) * 4 + x, (tp + dc) % 2


def moe_kernel(
    normed_ref, stream_ref, ids_ref, mix_ref, wg_hbm, wu_hbm, wd_hbm,
    out_ref,
    wg, wu, wd, sendbuf, recvbuf, ysend, yrecv, xs, hid, gates, wt_hi, wt_lo, acc,
    wsem, dsend, drecv, rsend, rrecv,
):
    sp, tp = lax.axis_index("sp"), lax.axis_index("tp")
    weights = [
        pltpu.make_async_copy(wg_hbm, wg, wsem.at[0]),
        pltpu.make_async_copy(wu_hbm, wu, wsem.at[1]),
        pltpu.make_async_copy(wd_hbm, wd, wsem.at[2]),
    ]
    for copy in weights:
        copy.start()
    barrier = pltpu.get_barrier_semaphore()

    def greet(i, carry):
        pl.semaphore_signal(barrier, inc=1, device_id=device_at(i, 1), device_id_type=MESH)
        return carry

    lax.fori_loop(1, N, greet, 0)

    slot = lax.broadcasted_iota(jnp.int32, (N, CAP * N), 1)
    i, r = slot // CAP, slot % CAP
    dz, dy, dx, dc = offsets(i)
    z, y, x = (sp // 16 + dz) % 4, ((sp // 4) % 4 + dy) % 4, (sp % 4 + dx) % 4
    expert = ((z * 4 + y) * 4 + x) * 2 + (tp + dc) % 2
    first = ids_ref[:, 0:1] == expert
    second = ids_ref[:, 1:2] == expert
    named = jnp.where(first | second, 1.0, 0.0)
    rows = lax.broadcasted_iota(jnp.int32, (N, N), 0)
    cols = lax.broadcasted_iota(jnp.int32, (N, N), 1)
    before = jnp.where(cols < rows, 1.0, 0.0).astype(BF)
    rank = jnp.dot(before, named.astype(BF), preferred_element_type=F32)
    chosen = jnp.where(rank == r.astype(F32), named, 0.0)
    gates[...] = jnp.transpose(chosen).astype(BF)
    weight = chosen * jnp.where(first, mix_ref[:, 0:1], mix_ref[:, 1:2])
    high = weight.astype(BF)
    wt_hi[...] = high
    wt_lo[...] = (weight - high.astype(F32)).astype(BF)

    def fill(g, carry):
        lhs = gates[pl.ds(pl.multiple_of(g * 128, 128), 128), :]
        for k in range(4):
            part = jnp.dot(
                lhs, normed_ref[:, k * TILE:(k + 1) * TILE], preferred_element_type=F32
            ).astype(BF)
            sendbuf[pl.ds(g * 32, 32), :, k * TILE:(k + 1) * TILE] = part.reshape(32, CAP, TILE)
        return carry

    lax.fori_loop(0, 4, fill, 0)
    recvbuf[0] = sendbuf[0]
    pl.semaphore_wait(barrier, N - 1)

    def dispatch(chunk):
        def one(i, carry):
            pltpu.make_async_remote_copy(
                src_ref=sendbuf.at[i], dst_ref=recvbuf.at[i],
                send_sem=dsend, recv_sem=drecv.at[chunk],
                device_id=device_at(i, 1), device_id_type=MESH,
            ).start()
            return carry

        lax.fori_loop(max(1, chunk * HALF), (chunk + 1) * HALF, one, 0)

    def giveback(chunk):
        def one(i, carry):
            pltpu.make_async_remote_copy(
                src_ref=ysend.at[i], dst_ref=yrecv.at[i],
                send_sem=rsend, recv_sem=rrecv.at[chunk],
                device_id=device_at(i, -1), device_id_type=MESH,
            ).start()
            return carry

        lax.fori_loop(max(1, chunk * HALF), (chunk + 1) * HALF, one, 0)

    def whole(chunk, source, target, send, recv):
        low = max(1, chunk * HALF)
        span = pl.ds(low, (chunk + 1) * HALF - low)
        return pltpu.make_async_remote_copy(
            src_ref=source.at[span], dst_ref=target.at[span], send_sem=send,
            recv_sem=recv.at[chunk], device_id=device_at(1, 1), device_id_type=MESH,
        )

    dispatch(0)
    dispatch(1)
    rows_chunk = HALF * CAP
    for chunk in range(2):
        whole(chunk, sendbuf, recvbuf, dsend, drecv).wait_recv()
        if chunk == 0:
            for copy in weights:
                copy.wait()

        def gather(g, carry):
            span = pl.ds(pl.multiple_of(g * 64, 64), 64)
            xs[span, :] = recvbuf[pl.ds(chunk * HALF + g * 16, 16)].reshape(64, 2048)
            return carry

        lax.fori_loop(0, 4, gather, 0)

        def up(j, carry):
            col = pl.ds(pl.multiple_of(j * TILE, TILE), TILE)
            gate = jnp.dot(xs[...], wg[:, col], preferred_element_type=F32)
            value = jnp.dot(xs[...], wu[:, col], preferred_element_type=F32)
            hid[:, col] = (gate * jax.nn.sigmoid(gate) * value).astype(BF)
            return carry

        lax.fori_loop(0, 1024 // TILE, up, 0)

        def down(j, carry):
            col = pl.ds(pl.multiple_of(j * TILE, TILE), TILE)
            part = jnp.dot(hid[...], wd[:, col], preferred_element_type=F32).astype(BF)
            ysend[chunk * HALF:(chunk + 1) * HALF, :, col] = part.reshape(HALF, CAP, TILE)
            return carry

        lax.fori_loop(0, 2048 // TILE, down, 0)
        if chunk == 0:
            yrecv[0] = ysend[0]
        giveback(chunk)

    for chunk in range(2):
        whole(chunk, ysend, yrecv, rsend, rrecv).wait_recv()
        slots = slice(chunk * rows_chunk, (chunk + 1) * rows_chunk)
        lhs_hi, lhs_lo = wt_hi[:, slots], wt_lo[:, slots]

        def combine(j, carry):
            col = pl.ds(pl.multiple_of(j * TILE, TILE), TILE)
            got = yrecv[chunk * HALF:(chunk + 1) * HALF, :, col].reshape(rows_chunk, TILE)
            part = jnp.dot(lhs_hi, got, preferred_element_type=F32)
            part = part + jnp.dot(lhs_lo, got, preferred_element_type=F32)
            if chunk == 0:
                acc[:, col] = part + stream_ref[:, col].astype(F32)
            else:
                out_ref[:, col] = (acc[:, col] + part).astype(BF)
            return carry

        lax.fori_loop(0, 2048 // TILE, combine, 0)
    for chunk in range(2):
        whole(chunk, sendbuf, recvbuf, dsend, drecv).wait_send()
        whole(chunk, ysend, yrecv, rsend, rrecv).wait_send()


def moe(normed, stream, ids, mix, w_gate, w_up, w_down):
    vmem = pl.BlockSpec(memory_space=pltpu.VMEM)
    hbm = pl.BlockSpec(memory_space=pltpu.HBM)
    slots = pltpu.VMEM((N, CAP, 2048), BF)
    return pl.pallas_call(
        moe_kernel,
        out_shape=jax.ShapeDtypeStruct((N, 2048), BF),
        in_specs=[vmem, vmem, vmem, vmem, hbm, hbm, hbm],
        out_specs=vmem,
        scratch_shapes=[
            pltpu.VMEM((2048, 1024), BF),
            pltpu.VMEM((2048, 1024), BF),
            pltpu.VMEM((1024, 2048), BF),
            slots, slots, slots, slots,
            pltpu.VMEM((HALF * CAP, 2048), BF),
            pltpu.VMEM((HALF * CAP, 1024), BF),
            pltpu.VMEM((CAP * N, N), BF),
            pltpu.VMEM((N, CAP * N), BF),
            pltpu.VMEM((N, CAP * N), BF),
            pltpu.VMEM((N, 2048), F32),
            pltpu.SemaphoreType.DMA((3,)),
            pltpu.SemaphoreType.DMA,
            pltpu.SemaphoreType.DMA((2,)),
            pltpu.SemaphoreType.DMA,
            pltpu.SemaphoreType.DMA((2,)),
        ],
        compiler_params=pltpu.CompilerParams(
            collective_id=0, has_side_effects=True, vmem_limit_bytes=56 * 2**20
        ),
        name="moe",
    )(normed, stream, ids, mix, w_gate, w_up, w_down)


def per_device(
    resid,
    value_in,
    gate_in,
    conv_weight,
    norm_gain,
    out_weight,
    ffn_gain,
    expert_ids,
    expert_mix,
    w_gate,
    w_up,
    w_down,
):
    glu = (value_in.astype(F32) * jax.nn.sigmoid(gate_in.astype(F32))).astype(BF)
    taps = conv_weight.shape[0]
    reach = taps // 2
    length = glu.shape[0]
    local_width = glu.shape[1]
    padded = padded_2(glu, (("sp", 0),), reach).astype(F32)
    conv = jnp.zeros((length, local_width), F32)
    for tap in range(taps):
        conv = conv + padded[tap : tap + length] * conv_weight[tap]
    sums = lax.psum((jnp.sum(conv, axis=1), jnp.sum(conv * conv, axis=1)), "tp")
    width = local_width * lax.axis_size("tp")
    mean = sums[0] / width
    var = sums[1] / width - mean * mean
    normed_conv = (conv - mean[:, None]) * lax.rsqrt(var + 1e-05)[:, None] * norm_gain
    mixed = jax.nn.silu(normed_conv).astype(BF)
    regrouped = lax.all_to_all(mixed, "tp", split_axis=0, concat_axis=1, tiled=True)
    proj = jnp.dot(regrouped, out_weight, preferred_element_type=F32)
    stream = (resid.astype(F32) + proj).astype(BF)
    wide = stream.astype(F32)
    normed = (
        wide * lax.rsqrt(jnp.mean(wide * wide, axis=1, keepdims=True) + 1e-06) * ffn_gain
    ).astype(BF)
    return moe(normed, stream, expert_ids, expert_mix, w_gate[0], w_up[0], w_down[0])


def solution(mesh):
    return jax.shard_map(
        per_device,
        mesh=mesh,
        in_specs=(
            P(("sp", "tp"), None),
            P("sp", "tp"),
            P("sp", "tp"),
            P(None, "tp"),
            P("tp"),
            P(),
            P(),
            P(("sp", "tp"), None),
            P(("sp", "tp"), None),
            P(("sp", "tp"), None, None),
            P(("sp", "tp"), None, None),
            P(("sp", "tp"), None, None),
        ),
        out_specs=P(("sp", "tp"), None),
        check_vma=False,
    )
```

```python
import functools

import jax
import jax.numpy as jnp
from jax import lax
from jax.experimental import pallas as pl
from jax.experimental.pallas import tpu as pltpu
from jax.sharding import PartitionSpec as P

MESH = pl.DeviceIdType.MESH
BF = jnp.bfloat16
F32 = jnp.float32
CAP = 4
N = 128
HALF = 64
TILE = 512


def offsets(i):
    a, b, c = i % 4, (i // 4) % 4, (i // 16) % 4
    return a, (a + b) % 4, (a + b + c) % 4, i // 64


def device_at(i, sign):
    sp, tp = lax.axis_index("sp"), lax.axis_index("tp")
    dz, dy, dx, dc = offsets(i)
    z, y, x = sp // 16, (sp // 4) % 4, sp % 4
    z, y, x = (z + 4 + sign * dz) % 4, (y + 4 + sign * dy) % 4, (x + 4 + sign * dx) % 4
    return (z * 4 + y) * 4 + x, (tp + dc) % 2


def device_in_line(dz, dy, dx, dc):
    sp, tp = lax.axis_index("sp"), lax.axis_index("tp")
    z, y, x = (sp // 16 + dz) % 4, ((sp // 4) % 4 + dy) % 4, (sp % 4 + dx) % 4
    return (z * 4 + y) * 4 + x, (tp + dc) % 2


def layer_kernel(
    resid_hbm, value_ref, gate_ref, taps_in, gain_in, ow_hbm, ffn_gain_ref, ids_ref, mix_ref,
    wg_hbm, wu_hbm, wd_hbm,
    out_ref,
    wg, wu, wd, ow, resid, taps, taps_other, gain_other, glu, other, halo, padded, conv, mixed, stream, normed,
    sendbuf, recvbuf, ysend, yrecv, xs, hid, gates, wt_hi, wt_lo, acc,
    wsem, tsend, trecv, gsend, grecv, hsend, hrecv, dsend, drecv, rsend, rrecv, y_ready, z_ready,
):
    sp, tp = lax.axis_index("sp"), lax.axis_index("tp")
    barrier = pltpu.get_barrier_semaphore()

    def signal(semaphore, device):
        pl.semaphore_signal(semaphore, inc=1, device_id=device, device_id_type=MESH)

    for dc in range(2):
        for dx in range(4):
            if dx or dc:
                signal(barrier, device_in_line(0, 0, dx, dc))
    for step in range(1, 4):
        signal(barrier, device_in_line(0, step, 0, 0))
        signal(barrier, device_in_line(step, 0, 0, 0))
    halo_from = jnp.where(tp == 0, sp - 1, sp + 1)
    has_halo = (halo_from >= 0) & (halo_from < 64)

    @pl.when(has_halo)
    def _():
        signal(barrier, (halo_from, 0))
        signal(barrier, (halo_from, 1))

    resid_copy = pltpu.make_async_copy(resid_hbm, resid, wsem.at[0])
    ow_copy = pltpu.make_async_copy(ow_hbm, ow, wsem.at[1])
    weights = [
        pltpu.make_async_copy(wg_hbm, wg, wsem.at[2]),
        pltpu.make_async_copy(wu_hbm, wu, wsem.at[3]),
        pltpu.make_async_copy(wd_hbm, wd, wsem.at[4]),
    ]
    for copy in [ow_copy, resid_copy] + weights:
        copy.start()

    def gated(g, carry):
        span = pl.ds(pl.multiple_of(g * 32, 32), 32)
        value = value_ref[span, :].astype(F32)
        glu[span, :] = (value * jax.nn.sigmoid(gate_ref[span, :].astype(F32))).astype(BF)
        return carry

    lax.fori_loop(0, 8, gated, 0)
    expected = 13 + jnp.where(sp > 0, 1, 0) + jnp.where(sp < 63, 1, 0)
    pl.semaphore_wait(barrier, expected)

    peer_rows = pl.ds(pl.multiple_of(112 * (1 - tp), 16), 144)
    to_peer = pltpu.make_async_remote_copy(
        src_ref=glu.at[peer_rows], dst_ref=other, send_sem=gsend, recv_sem=grecv,
        device_id=(sp, 1 - tp), device_id_type=MESH,
    )
    to_peer.start()
    taps_to_peer = pltpu.make_async_remote_copy(
        src_ref=taps_in, dst_ref=taps_other, send_sem=tsend.at[0], recv_sem=trecv.at[0],
        device_id=(sp, 1 - tp), device_id_type=MESH,
    )
    taps_to_peer.start()
    gain_to_peer = pltpu.make_async_remote_copy(
        src_ref=gain_in, dst_ref=gain_other, send_sem=tsend.at[1], recv_sem=trecv.at[1],
        device_id=(sp, 1 - tp), device_id_type=MESH,
    )
    gain_to_peer.start()
    to_next = pltpu.make_async_remote_copy(
        src_ref=glu.at[pl.ds(240, 16)], dst_ref=halo.at[tp], send_sem=hsend.at[0],
        recv_sem=hrecv.at[tp], device_id=(sp + 1, 0), device_id_type=MESH,
    )
    to_previous = pltpu.make_async_remote_copy(
        src_ref=glu.at[pl.ds(0, 16)], dst_ref=halo.at[tp], send_sem=hsend.at[1],
        recv_sem=hrecv.at[tp], device_id=(sp - 1, 1), device_id_type=MESH,
    )

    @pl.when(sp < 63)
    def _():
        to_next.start()

    @pl.when(sp > 0)
    def _():
        to_previous.start()

    for step in range(1, 4):
        signal(y_ready, device_in_line(0, step, 0, 0))

    own_rows = pl.multiple_of(112 * tp, 16)
    inner = pl.multiple_of(16 * (1 - tp), 16)
    edge = pl.multiple_of(144 * tp, 16)
    edge_out = pl.multiple_of(112 * tp, 16)
    for k in range(6):
        lanes = slice(k * 128, (k + 1) * 128)
        padded[tp * 6 + k, pl.ds(inner, 144), :] = glu[pl.ds(own_rows, 144), lanes].astype(F32)
        taps[tp * 6 + k, 0:31, :] = taps_in[:, lanes]
        taps[tp * 6 + k, 31:32, :] = gain_in[lanes].reshape(1, 128)

    def convolve(block, start, count):
        total = jnp.zeros((count, 128), F32)
        for tap in range(31):
            total = total + padded[block, pl.ds(start + tap + 1, count), :] * taps[block, tap:tap + 1, :]
        conv[block, pl.ds(start, count), :] = total

    def inner_blocks(first):
        def one(k, carry):
            convolve(first + k, inner, 56)
            convolve(first + k, inner + 56, 56)
            return carry

        lax.fori_loop(0, 6, one, 0)

    inner_blocks(tp * 6)
    to_peer.wait_recv()
    taps_to_peer.wait_recv()
    gain_to_peer.wait_recv()
    for k in range(6):
        lanes = slice(k * 128, (k + 1) * 128)
        padded[(1 - tp) * 6 + k, pl.ds(inner, 144), :] = other[:, lanes].astype(F32)
        taps[(1 - tp) * 6 + k, 0:31, :] = taps_other[:, lanes]
        taps[(1 - tp) * 6 + k, 31:32, :] = gain_other[lanes].reshape(1, 128)
    pl.semaphore_wait(y_ready, 3)
    for step in range(1, 4):
        signal(z_ready, device_in_line(step, 0, 0, 0))
    inner_blocks((1 - tp) * 6)

    @pl.when(has_halo)
    def _():
        for c in range(2):
            pltpu.make_async_remote_copy(
                src_ref=glu.at[pl.ds(0, 16)], dst_ref=halo.at[c], send_sem=hsend.at[0],
                recv_sem=hrecv.at[c], device_id=(sp, 1 - tp), device_id_type=MESH,
            ).wait_recv()
            for k in range(6):
                lanes = slice(k * 128, (k + 1) * 128)
                padded[c * 6 + k, pl.ds(edge, 16), :] = halo[c, :, lanes].astype(F32)

    @pl.when(jnp.logical_not(has_halo))
    def _():
        for k in range(12):
            padded[k, pl.ds(edge, 16), :] = jnp.zeros((16, 128), F32)

    def edges(k, carry):
        convolve(k, edge_out, 16)
        return carry

    lax.fori_loop(0, 12, edges, 0)

    def channel_norm(g, carry):
        span = pl.ds(pl.multiple_of(g * 32, 32), 32)
        total = jnp.zeros((32, 128), F32)
        square = jnp.zeros((32, 128), F32)
        for k in range(12):
            part = conv[k, span, :]
            total = total + part
            square = square + part * part
        mean = jnp.sum(total, axis=1, keepdims=True) / 1536
        var = jnp.sum(square, axis=1, keepdims=True) / 1536 - mean * mean
        scale = lax.rsqrt(var + 1e-05)
        for k in range(12):
            part = (conv[k, span, :] - mean) * scale * taps[k, 31:32, :]
            mixed[span, k * 128:(k + 1) * 128] = (part * jax.nn.sigmoid(part)).astype(BF)
        return carry

    lax.fori_loop(0, 4, channel_norm, 0)

    slot = lax.broadcasted_iota(jnp.int32, (CAP * N, N), 0)
    i, r = slot // CAP, slot % CAP
    dz, dy, dx, dc = offsets(i)
    z, y, x = (sp // 16 + dz) % 4, ((sp // 4) % 4 + dy) % 4, (sp % 4 + dx) % 4
    expert = ((z * 4 + y) * 4 + x) * 2 + (tp + dc) % 2
    first = ids_ref[0:1, :] == expert
    second = ids_ref[1:2, :] == expert
    named = jnp.where(first | second, 1.0, 0.0)
    rows = lax.broadcasted_iota(jnp.int32, (N, N), 0)
    cols = lax.broadcasted_iota(jnp.int32, (N, N), 1)
    before = jnp.where(rows < cols, 1.0, 0.0).astype(BF)
    rank = jnp.dot(named.astype(BF), before, preferred_element_type=F32)
    chosen = jnp.where(rank == r.astype(F32), named, 0.0)
    gates[...] = chosen.astype(BF)
    weight = jnp.transpose(chosen * jnp.where(first, mix_ref[0:1, :], mix_ref[1:2, :]))
    high = weight.astype(BF)
    wt_hi[...] = high
    wt_lo[...] = (weight - high.astype(F32)).astype(BF)

    resid_copy.wait()
    ow_copy.wait()

    def project(j, squares):
        col = pl.ds(pl.multiple_of(j * TILE, TILE), TILE)
        part = jnp.dot(mixed[...], ow[:, col], preferred_element_type=F32)
        total = (resid[:, col].astype(F32) + part).astype(BF)
        stream[:, col] = total
        wide = total.astype(F32)
        return squares + jnp.sum(wide * wide, axis=1, keepdims=True)

    squares = lax.fori_loop(0, 4, project, jnp.zeros((N, 1), F32))
    scale = lax.rsqrt(squares / 2048 + 1e-06)

    def fill(k, carry):
        col = pl.ds(pl.multiple_of(k * TILE, TILE), TILE)
        normed = (stream[:, col].astype(F32) * scale * ffn_gain_ref[:, col]).astype(BF)
        for g in range(4):
            part = jnp.dot(
                gates[g * 128:(g + 1) * 128, :], normed, preferred_element_type=F32
            ).astype(BF)
            sendbuf[g * 32:(g + 1) * 32, :, col] = part.reshape(32, CAP, TILE)
        return carry

    lax.fori_loop(0, 4, fill, 0)
    recvbuf[0] = sendbuf[0]
    pl.semaphore_wait(z_ready, 3)

    def dispatch(chunk):
        def one(i, carry):
            pltpu.make_async_remote_copy(
                src_ref=sendbuf.at[i], dst_ref=recvbuf.at[i],
                send_sem=dsend, recv_sem=drecv.at[chunk],
                device_id=device_at(i, 1), device_id_type=MESH,
            ).start()
            return carry

        lax.fori_loop(max(1, chunk * HALF), (chunk + 1) * HALF, one, 0)

    def giveback(chunk):
        def one(i, carry):
            pltpu.make_async_remote_copy(
                src_ref=ysend.at[i], dst_ref=yrecv.at[i],
                send_sem=rsend, recv_sem=rrecv.at[chunk],
                device_id=device_at(i, -1), device_id_type=MESH,
            ).start()
            return carry

        lax.fori_loop(max(1, chunk * HALF), (chunk + 1) * HALF, one, 0)

    def whole(chunk, source, target, send, recv):
        low = max(1, chunk * HALF)
        span = pl.ds(low, (chunk + 1) * HALF - low)
        return pltpu.make_async_remote_copy(
            src_ref=source.at[span], dst_ref=target.at[span], send_sem=send,
            recv_sem=recv.at[chunk], device_id=device_at(1, 1), device_id_type=MESH,
        )

    dispatch(0)
    dispatch(1)
    rows_chunk = HALF * CAP
    for chunk in range(2):
        whole(chunk, sendbuf, recvbuf, dsend, drecv).wait_recv()
        if chunk == 0:
            for copy in weights:
                copy.wait()

        def gather(g, carry):
            span = pl.ds(pl.multiple_of(g * 64, 64), 64)
            xs[span, :] = recvbuf[pl.ds(chunk * HALF + g * 16, 16)].reshape(64, 2048)
            return carry

        lax.fori_loop(0, 4, gather, 0)

        def up(j, carry):
            col = pl.ds(pl.multiple_of(j * TILE, TILE), TILE)
            gate = jnp.dot(xs[...], wg[:, col], preferred_element_type=F32)
            value = jnp.dot(xs[...], wu[:, col], preferred_element_type=F32)
            hid[:, col] = (gate * jax.nn.sigmoid(gate) * value).astype(BF)
            return carry

        lax.fori_loop(0, 1024 // TILE, up, 0)

        def down(j, carry):
            col = pl.ds(pl.multiple_of(j * TILE, TILE), TILE)
            part = jnp.dot(hid[...], wd[:, col], preferred_element_type=F32).astype(BF)
            ysend[chunk * HALF:(chunk + 1) * HALF, :, col] = part.reshape(HALF, CAP, TILE)
            return carry

        lax.fori_loop(0, 2048 // TILE, down, 0)
        if chunk == 0:
            yrecv[0] = ysend[0]
        giveback(chunk)

    for chunk in range(2):
        whole(chunk, ysend, yrecv, rsend, rrecv).wait_recv()
        slots = slice(chunk * rows_chunk, (chunk + 1) * rows_chunk)
        lhs_hi, lhs_lo = wt_hi[:, slots], wt_lo[:, slots]

        def combine(j, carry):
            col = pl.ds(pl.multiple_of(j * TILE, TILE), TILE)
            got = yrecv[chunk * HALF:(chunk + 1) * HALF, :, col].reshape(rows_chunk, TILE)
            part = jnp.dot(lhs_hi, got, preferred_element_type=F32)
            part = part + jnp.dot(lhs_lo, got, preferred_element_type=F32)
            if chunk == 0:
                acc[:, col] = part + stream[:, col].astype(F32)
            else:
                out_ref[:, col] = acc[:, col] + part
            return carry

        lax.fori_loop(0, 2048 // TILE, combine, 0)
    for chunk in range(2):
        whole(chunk, sendbuf, recvbuf, dsend, drecv).wait_send()
        whole(chunk, ysend, yrecv, rsend, rrecv).wait_send()
    to_peer.wait_send()
    taps_to_peer.wait_send()
    gain_to_peer.wait_send()

    @pl.when(sp < 63)
    def _():
        to_next.wait_send()

    @pl.when(sp > 0)
    def _():
        to_previous.wait_send()


def per_device(
    resid,
    value_in,
    gate_in,
    conv_weight,
    norm_gain,
    out_weight,
    ffn_gain,
    expert_ids,
    expert_mix,
    w_gate,
    w_up,
    w_down,
):
    vmem = pl.BlockSpec(memory_space=pltpu.VMEM)
    hbm = pl.BlockSpec(memory_space=pltpu.HBM)
    slots = pltpu.VMEM((N, CAP, 2048), BF)
    dma = pltpu.SemaphoreType.DMA
    total = pl.pallas_call(
        layer_kernel,
        out_shape=jax.ShapeDtypeStruct((N, 2048), F32),
        in_specs=[hbm, vmem, vmem, vmem, vmem, hbm, vmem, vmem, vmem, hbm, hbm, hbm],
        out_specs=vmem,
        scratch_shapes=[
            pltpu.VMEM((2048, 1024), BF),
            pltpu.VMEM((2048, 1024), BF),
            pltpu.VMEM((1024, 2048), BF),
            pltpu.VMEM((1536, 2048), BF),
            pltpu.VMEM((N, 2048), BF),
            pltpu.VMEM((12, 32, 128), F32),
            pltpu.VMEM((31, 768), F32),
            pltpu.VMEM((768,), F32),
            pltpu.VMEM((256, 768), BF),
            pltpu.VMEM((144, 768), BF),
            pltpu.VMEM((2, 16, 768), BF),
            pltpu.VMEM((12, 160, 128), F32),
            pltpu.VMEM((12, 128, 128), F32),
            pltpu.VMEM((N, 1536), BF),
            pltpu.VMEM((N, 2048), BF),
            pltpu.VMEM((N, 2048), BF),
            slots, slots, slots, slots,
            pltpu.VMEM((HALF * CAP, 2048), BF),
            pltpu.VMEM((HALF * CAP, 1024), BF),
            pltpu.VMEM((CAP * N, N), BF),
            pltpu.VMEM((N, CAP * N), BF),
            pltpu.VMEM((N, CAP * N), BF),
            pltpu.VMEM((N, 2048), F32),
            dma((5,)), dma((2,)), dma((2,)), dma, dma, dma((2,)), dma((2,)), dma, dma((2,)), dma, dma((2,)),
            pltpu.SemaphoreType.REGULAR, pltpu.SemaphoreType.REGULAR,
        ],
        compiler_params=pltpu.CompilerParams(
            collective_id=0, has_side_effects=True, vmem_limit_bytes=60 * 2**20
        ),
        name="layer",
    )(
        resid, value_in, gate_in, conv_weight, norm_gain, out_weight,
        ffn_gain.reshape(1, 2048), expert_ids.T, expert_mix.T, w_gate[0], w_up[0], w_down[0],
    )
    return total.astype(BF)


def solution(mesh):
    return jax.shard_map(
        per_device,
        mesh=mesh,
        in_specs=(
            P(("sp", "tp"), None),
            P("sp", "tp"),
            P("sp", "tp"),
            P(None, "tp"),
            P("tp"),
            P(),
            P(),
            P(("sp", "tp"), None),
            P(("sp", "tp"), None),
            P(("sp", "tp"), None, None),
            P(("sp", "tp"), None, None),
            P(("sp", "tp"), None, None),
        ),
        out_specs=P(("sp", "tp"), None),
        check_vma=False,
    )
```

```python
import functools

import jax
import jax.numpy as jnp
from jax import lax
from jax.experimental import pallas as pl
from jax.experimental.pallas import tpu as pltpu
from jax.sharding import PartitionSpec as P

MESH = pl.DeviceIdType.MESH
BF = jnp.bfloat16
F32 = jnp.float32
CAP = 4
N = 128
TILE = 512
CHUNKS = 4
PEERS = N // CHUNKS
ROWS = PEERS * CAP


def offsets(i):
    a, b, c = i % 4, (i // 4) % 4, (i // 16) % 4
    return a, (a + b) % 4, (a + b + c) % 4, i // 64


def device_at(i, sign):
    sp, tp = lax.axis_index("sp"), lax.axis_index("tp")
    dz, dy, dx, dc = offsets(i)
    z, y, x = sp // 16, (sp // 4) % 4, sp % 4
    z, y, x = (z + 4 + sign * dz) % 4, (y + 4 + sign * dy) % 4, (x + 4 + sign * dx) % 4
    return (z * 4 + y) * 4 + x, (tp + dc) % 2


def device_in_line(dz, dy, dx, dc):
    sp, tp = lax.axis_index("sp"), lax.axis_index("tp")
    z, y, x = (sp // 16 + dz) % 4, ((sp // 4) % 4 + dy) % 4, (sp % 4 + dx) % 4
    return (z * 4 + y) * 4 + x, (tp + dc) % 2


def layer_kernel(
    resid_hbm, value_hbm, gate_hbm, taps_hbm, gain_hbm, ow_hbm, ffn_gain_hbm, ids_hbm, mix_hbm,
    wg_hbm, wu_hbm, wd_hbm,
    out_ref,
    value, gate, taps_in, gain_in, ffn_gain, ids, mix, resid, ow, wg, wu, wd,
    taps, taps_other, gain_other, glu, other, halo, padded, conv, mixed, stream, normed,
    sendbuf, recvbuf, ysend, yrecv, xs, hid, gates, wt, acc,
    insem, gsend, grecv, hsend, hrecv, dsend, drecv, rsend, rrecv, y_ready, z_ready,
):
    sp, tp = lax.axis_index("sp"), lax.axis_index("tp")
    barrier = pltpu.get_barrier_semaphore()

    def signal(semaphore, device):
        pl.semaphore_signal(semaphore, inc=1, device_id=device, device_id_type=MESH)

    halo_from = jnp.where(tp == 0, sp - 1, sp + 1)
    has_halo = (halo_from >= 0) & (halo_from < 64)

    @pl.when(has_halo)
    def _():
        signal(barrier, (halo_from, 0))
        signal(barrier, (halo_from, 1))

    for step in (2, 3, 1):
        signal(barrier, device_in_line(0, step, 0, 0))
        signal(barrier, device_in_line(step, 0, 0, 0))
    for dc in range(2):
        for dx in range(4):
            if dx or dc:
                signal(barrier, device_in_line(0, 0, dx, dc))

    fetched = [
        pltpu.make_async_copy(source, target, insem.at[n])
        for n, (source, target) in enumerate([
            (value_hbm, value), (gate_hbm, gate), (taps_hbm, taps_in), (gain_hbm, gain_in),
            (ids_hbm, ids), (mix_hbm, mix), (ffn_gain_hbm, ffn_gain), (resid_hbm, resid),
            (ow_hbm, ow), (wg_hbm, wg), (wu_hbm, wu), (wd_hbm, wd),
        ])
    ]
    for copy in fetched:
        copy.start()
    for copy in fetched[:4]:
        copy.wait()

    def gated(g, carry):
        span = pl.ds(pl.multiple_of(g * 32, 32), 32)
        wide = value[span, :].astype(F32)
        glu[span, :] = (wide * jax.nn.sigmoid(gate[span, :].astype(F32))).astype(BF)
        return carry

    lax.fori_loop(0, 8, gated, 0)

    own_rows = pl.multiple_of(112 * tp, 16)
    inner = pl.multiple_of(16 * (1 - tp), 16)
    edge = pl.multiple_of(144 * tp, 16)
    inner_out = inner
    edge_out = pl.multiple_of(112 * tp, 16)

    def place(first, rows_of, taps_of, gain_of):
        for k in range(6):
            lanes = slice(k * 128, (k + 1) * 128)
            padded[first + k, pl.ds(inner, 144), :] = rows_of(lanes).astype(F32)
            taps[first + k, 0:31, :] = taps_of[:, lanes]
            taps[first + k, 31:32, :] = gain_of[lanes].reshape(1, 128)

    def convolve(block, start, count):
        total = jnp.zeros((count, 128), F32)
        for tap in range(31):
            total = total + padded[block, pl.ds(start + tap + 1, count), :] * taps[
                block, tap:tap + 1, :
            ]
        conv[block, pl.ds(start, count), :] = total

    def inner_blocks(first):
        def one(k, carry):
            convolve(first + k, inner_out, 56)
            convolve(first + k, inner_out + 56, 56)
            return carry

        lax.fori_loop(0, 6, one, 0)

    place(tp * 6, lambda lanes: glu[pl.ds(own_rows, 144), lanes], taps_in, gain_in)
    inner_blocks(tp * 6)
    expected = 13 + jnp.where(sp > 0, 1, 0) + jnp.where(sp < 63, 1, 0)
    pl.semaphore_wait(barrier, expected)

    to_next = pltpu.make_async_remote_copy(
        src_ref=glu.at[pl.ds(240, 16)], dst_ref=halo.at[tp], send_sem=hsend.at[0],
        recv_sem=hrecv.at[tp], device_id=(sp + 1, 0), device_id_type=MESH,
    )
    to_previous = pltpu.make_async_remote_copy(
        src_ref=glu.at[pl.ds(0, 16)], dst_ref=halo.at[tp], send_sem=hsend.at[1],
        recv_sem=hrecv.at[tp], device_id=(sp - 1, 1), device_id_type=MESH,
    )

    @pl.when(sp < 63)
    def _():
        to_next.start()

    @pl.when(sp > 0)
    def _():
        to_previous.start()

    for step in (2, 3, 1):
        signal(y_ready, device_in_line(0, step, 0, 0))
    peer_rows = pl.ds(pl.multiple_of(112 * (1 - tp), 16), 144)
    to_peer = [
        pltpu.make_async_remote_copy(
            src_ref=source, dst_ref=target, send_sem=gsend.at[n], recv_sem=grecv.at[n],
            device_id=(sp, 1 - tp), device_id_type=MESH,
        )
        for n, (source, target) in enumerate(
            [(glu.at[peer_rows], other), (taps_in, taps_other), (gain_in, gain_other)]
        )
    ]
    for copy in to_peer:
        copy.start()
    for copy in fetched[4:6]:
        copy.wait()

    slot = lax.broadcasted_iota(jnp.int32, (CAP * N, N), 0)
    i, r = slot // CAP, slot % CAP
    dz, dy, dx, dc = offsets(i)
    z, y, x = (sp // 16 + dz) % 4, ((sp // 4) % 4 + dy) % 4, (sp % 4 + dx) % 4
    expert = ((z * 4 + y) * 4 + x) * 2 + (tp + dc) % 2
    first = ids[0:1, :] == expert
    second = ids[1:2, :] == expert
    named = jnp.where(first | second, 1.0, 0.0)
    rows = lax.broadcasted_iota(jnp.int32, (N, N), 0)
    cols = lax.broadcasted_iota(jnp.int32, (N, N), 1)
    before = jnp.where(rows < cols, 1.0, 0.0).astype(BF)
    rank = jnp.dot(named.astype(BF), before, preferred_element_type=F32)
    chosen = jnp.where(rank == r.astype(F32), named, 0.0)
    gates[...] = chosen.astype(BF)
    weight = jnp.transpose(chosen * jnp.where(first, mix[0:1, :], mix[1:2, :]))
    high = weight.astype(BF)
    wt[0:N, :] = high
    wt[N:2 * N, :] = (weight - high.astype(F32)).astype(BF)

    for copy in to_peer:
        copy.wait_recv()
    place((1 - tp) * 6, lambda lanes: other[:, lanes], taps_other, gain_other)
    inner_blocks((1 - tp) * 6)
    pl.semaphore_wait(y_ready, 3)
    for step in (2, 3, 1):
        signal(z_ready, device_in_line(step, 0, 0, 0))

    def channel_norm(start, count):
        span = pl.ds(start, count)
        total = jnp.zeros((count, 128), F32)
        square = jnp.zeros((count, 128), F32)
        for k in range(12):
            part = conv[k, span, :]
            total = total + part
            square = square + part * part
        mean = jnp.sum(total, axis=1, keepdims=True) / 1536
        var = jnp.sum(square, axis=1, keepdims=True) / 1536 - mean * mean
        scale = lax.rsqrt(var + 1e-05)
        for k in range(12):
            part = (conv[k, span, :] - mean) * scale * taps[k, 31:32, :]
            mixed[span, k * 128:(k + 1) * 128] = (part * jax.nn.sigmoid(part)).astype(BF)

    def inner_norm(g, carry):
        channel_norm(pl.multiple_of(inner_out + g * 16, 16), 16)
        return carry

    lax.fori_loop(0, 7, inner_norm, 0)

    @pl.when(has_halo)
    def _():
        for c in range(2):
            pltpu.make_async_remote_copy(
                src_ref=glu.at[pl.ds(0, 16)], dst_ref=halo.at[c], send_sem=hsend.at[0],
                recv_sem=hrecv.at[c], device_id=(sp, 1 - tp), device_id_type=MESH,
            ).wait_recv()
            for k in range(6):
                lanes = slice(k * 128, (k + 1) * 128)
                padded[c * 6 + k, pl.ds(edge, 16), :] = halo[c, :, lanes].astype(F32)

    @pl.when(jnp.logical_not(has_halo))
    def _():
        for k in range(12):
            padded[k, pl.ds(edge, 16), :] = jnp.zeros((16, 128), F32)

    def edges(k, carry):
        convolve(k, edge_out, 16)
        return carry

    lax.fori_loop(0, 12, edges, 0)
    channel_norm(edge_out, 16)
    for copy in fetched[6:9]:
        copy.wait()

    def project(j, squares):
        col = pl.ds(pl.multiple_of(j * TILE, TILE), TILE)
        part = jnp.dot(mixed[...], ow[:, col], preferred_element_type=F32)
        total = (resid[:, col].astype(F32) + part).astype(BF)
        stream[:, col] = total
        wide = total.astype(F32)
        return squares + jnp.sum(wide * wide, axis=1, keepdims=True)

    squares = lax.fori_loop(0, 4, project, jnp.zeros((N, 1), F32))
    scale = lax.rsqrt(squares / 2048 + 1e-06)
    for k in range(4):
        col = slice(k * TILE, (k + 1) * TILE)
        normed[:, col] = (stream[:, col].astype(F32) * scale * ffn_gain[:, col]).astype(BF)
    pl.semaphore_wait(z_ready, 3)

    def send_all(chunk, source, target, send, recv, sign):
        def one(i, carry):
            pltpu.make_async_remote_copy(
                src_ref=source.at[i], dst_ref=target.at[i], send_sem=send,
                recv_sem=recv.at[chunk], device_id=device_at(i, sign), device_id_type=MESH,
            ).start()
            return carry

        lax.fori_loop(max(1, chunk * PEERS), (chunk + 1) * PEERS, one, 0)

    def whole(chunk, source, target, send, recv):
        low = max(1, chunk * PEERS)
        span = pl.ds(low, (chunk + 1) * PEERS - low)
        return pltpu.make_async_remote_copy(
            src_ref=source.at[span], dst_ref=target.at[span], send_sem=send,
            recv_sem=recv.at[chunk], device_id=device_at(1, 1), device_id_type=MESH,
        )

    for chunk in range(CHUNKS):
        def fill(k, carry):
            col = pl.ds(pl.multiple_of(k * TILE, TILE), TILE)
            part = jnp.dot(
                gates[chunk * ROWS:(chunk + 1) * ROWS, :], normed[:, col],
                preferred_element_type=F32,
            ).astype(BF)
            sendbuf[chunk * PEERS:(chunk + 1) * PEERS, :, col] = part.reshape(PEERS, CAP, TILE)
            return carry

        lax.fori_loop(0, 4, fill, 0)
        send_all(chunk, sendbuf, recvbuf, dsend, drecv, 1)
    recvbuf[0] = sendbuf[0]
    for copy in fetched[9:]:
        copy.wait()

    for chunk in range(CHUNKS):
        whole(chunk, sendbuf, recvbuf, dsend, drecv).wait_recv()
        peers = slice(chunk * PEERS, (chunk + 1) * PEERS)
        xs[...] = recvbuf[peers].reshape(ROWS, 2048)

        def up(j, carry):
            col = pl.ds(pl.multiple_of(j * TILE, TILE), TILE)
            gated_part = jnp.dot(xs[...], wg[:, col], preferred_element_type=F32)
            up_part = jnp.dot(xs[...], wu[:, col], preferred_element_type=F32)
            hid[:, col] = (gated_part * jax.nn.sigmoid(gated_part) * up_part).astype(BF)
            return carry

        lax.fori_loop(0, 1024 // TILE, up, 0)

        def down(j, carry):
            col = pl.ds(pl.multiple_of(j * TILE, TILE), TILE)
            part = jnp.dot(hid[...], wd[:, col], preferred_element_type=F32).astype(BF)
            ysend[peers, :, col] = part.reshape(PEERS, CAP, TILE)
            return carry

        lax.fori_loop(0, 2048 // TILE, down, 0)
        if chunk == 0:
            yrecv[0] = ysend[0]
        send_all(chunk, ysend, yrecv, rsend, rrecv, -1)

    for chunk in range(CHUNKS):
        whole(chunk, ysend, yrecv, rsend, rrecv).wait_recv()
        peers = slice(chunk * PEERS, (chunk + 1) * PEERS)

        def combine(j, carry):
            col = pl.ds(pl.multiple_of(j * TILE, TILE), TILE)
            got = yrecv[peers, :, col].reshape(ROWS, TILE)
            both = jnp.dot(
                wt[:, chunk * ROWS:(chunk + 1) * ROWS], got, preferred_element_type=F32
            )
            part = both[0:N] + both[N:2 * N]
            if chunk == 0:
                acc[:, col] = part + stream[:, col].astype(F32)
            elif chunk < CHUNKS - 1:
                acc[:, col] = acc[:, col] + part
            else:
                out_ref[:, col] = acc[:, col] + part
            return carry

        lax.fori_loop(0, 2048 // TILE, combine, 0)

    for chunk in range(CHUNKS):
        whole(chunk, sendbuf, recvbuf, dsend, drecv).wait_send()
        whole(chunk, ysend, yrecv, rsend, rrecv).wait_send()
    for copy in to_peer:
        copy.wait_send()

    @pl.when(sp < 63)
    def _():
        to_next.wait_send()

    @pl.when(sp > 0)
    def _():
        to_previous.wait_send()


def per_device(
    resid,
    value_in,
    gate_in,
    conv_weight,
    norm_gain,
    out_weight,
    ffn_gain,
    expert_ids,
    expert_mix,
    w_gate,
    w_up,
    w_down,
):
    vmem = pl.BlockSpec(memory_space=pltpu.VMEM)
    hbm = pl.BlockSpec(memory_space=pltpu.HBM)
    slots = pltpu.VMEM((N, CAP, 2048), BF)
    dma = pltpu.SemaphoreType.DMA
    total = pl.pallas_call(
        layer_kernel,
        out_shape=pltpu.VMEM((N, 2048), F32),
        in_specs=[hbm] * 12,
        out_specs=vmem,
        scratch_shapes=[
            pltpu.VMEM((256, 768), BF),
            pltpu.VMEM((256, 768), BF),
            pltpu.VMEM((31, 768), F32),
            pltpu.VMEM((768,), F32),
            pltpu.VMEM((1, 2048), F32),
            pltpu.VMEM((2, N), jnp.int32),
            pltpu.VMEM((2, N), F32),
            pltpu.VMEM((N, 2048), BF),
            pltpu.VMEM((1536, 2048), BF),
            pltpu.VMEM((2048, 1024), BF),
            pltpu.VMEM((2048, 1024), BF),
            pltpu.VMEM((1024, 2048), BF),
            pltpu.VMEM((12, 32, 128), F32),
            pltpu.VMEM((31, 768), F32),
            pltpu.VMEM((768,), F32),
            pltpu.VMEM((256, 768), BF),
            pltpu.VMEM((144, 768), BF),
            pltpu.VMEM((2, 16, 768), BF),
            pltpu.VMEM((12, 160, 128), F32),
            pltpu.VMEM((12, 128, 128), F32),
            pltpu.VMEM((N, 1536), BF),
            pltpu.VMEM((N, 2048), BF),
            pltpu.VMEM((N, 2048), BF),
            slots, slots, slots, slots,
            pltpu.VMEM((ROWS, 2048), BF),
            pltpu.VMEM((ROWS, 1024), BF),
            pltpu.VMEM((CAP * N, N), BF),
            pltpu.VMEM((2 * N, CAP * N), BF),
            pltpu.VMEM((N, 2048), F32),
            dma((12,)), dma((3,)), dma((3,)), dma((2,)), dma((2,)), dma, dma((CHUNKS,)), dma,
            dma((CHUNKS,)), pltpu.SemaphoreType.REGULAR, pltpu.SemaphoreType.REGULAR,
        ],
        compiler_params=pltpu.CompilerParams(
            collective_id=0, has_side_effects=True, vmem_limit_bytes=60 * 2**20
        ),
        name="layer",
    )(
        resid, value_in, gate_in, conv_weight, norm_gain, out_weight,
        ffn_gain.reshape(1, 2048), expert_ids.T, expert_mix.T, w_gate[0], w_up[0], w_down[0],
    )
    return total.astype(BF)


def solution(mesh):
    return jax.shard_map(
        per_device,
        mesh=mesh,
        in_specs=(
            P(("sp", "tp"), None),
            P("sp", "tp"),
            P("sp", "tp"),
            P(None, "tp"),
            P("tp"),
            P(),
            P(),
            P(("sp", "tp"), None),
            P(("sp", "tp"), None),
            P(("sp", "tp"), None, None),
            P(("sp", "tp"), None, None),
            P(("sp", "tp"), None, None),
        ),
        out_specs=P(("sp", "tp"), None),
        check_vma=False,
    )
```

```python
import functools

import jax
import jax.numpy as jnp
from jax import lax
from jax.experimental import pallas as pl
from jax.experimental.pallas import tpu as pltpu
from jax.sharding import PartitionSpec as P

MESH = pl.DeviceIdType.MESH
BF = jnp.bfloat16
F32 = jnp.float32
CAP = 4
N = 128
TILE = 512
CHUNKS = 4
BACK = 4
PEERS = N // CHUNKS
ROWS = PEERS * CAP
GATHER = 256


def offsets(i):
    a, b, c = i % 4, (i // 4) % 4, (i // 16) % 4
    return a, (a + b) % 4, (a + b + c) % 4, i // 64


def sigmoid(v):
    return 0.5 * jnp.tanh(0.5 * v) + 0.5


def device_at(i, sign):
    sp, tp = lax.axis_index("sp"), lax.axis_index("tp")
    dz, dy, dx, dc = offsets(i)
    z, y, x = sp // 16, (sp // 4) % 4, sp % 4
    z, y, x = (z + 4 + sign * dz) % 4, (y + 4 + sign * dy) % 4, (x + 4 + sign * dx) % 4
    return (z * 4 + y) * 4 + x, (tp + dc) % 2


def device_in_line(dz, dy, dx, dc):
    sp, tp = lax.axis_index("sp"), lax.axis_index("tp")
    z, y, x = (sp // 16 + dz) % 4, ((sp // 4) % 4 + dy) % 4, (sp % 4 + dx) % 4
    return (z * 4 + y) * 4 + x, (tp + dc) % 2


def layer_kernel(
    resid_hbm, value_hbm, gate_hbm, taps_hbm, gain_hbm, ow_hbm, ffn_gain_hbm, ids_hbm, mix_hbm,
    wg_hbm, wu_hbm, wd_hbm,
    out_ref,
    value, gate, taps_in, gain_in, ffn_gain, ids, mix, resid, ow, wg, wu, wd,
    taps, taps_other, gain_other, glu, other, halo, padded, conv, mixed, stream,
    sendbuf, recvbuf, ysend, yrecv, xs, hid, gates, wt, acc,
    insem, gsend, grecv, hsend, hrecv, dsend, drecv, rsend, rrecv, y_ready, z_ready,
):
    sp, tp = lax.axis_index("sp"), lax.axis_index("tp")
    barrier = pltpu.get_barrier_semaphore()

    def signal(semaphore, device):
        pl.semaphore_signal(semaphore, inc=1, device_id=device, device_id_type=MESH)

    halo_from = jnp.where(tp == 0, sp - 1, sp + 1)
    has_halo = (halo_from >= 0) & (halo_from < 64)

    @pl.when(has_halo)
    def _():
        signal(barrier, (halo_from, 0))
        signal(barrier, (halo_from, 1))

    for step in (2, 3, 1):
        signal(barrier, device_in_line(0, step, 0, 0))
        signal(barrier, device_in_line(step, 0, 0, 0))
    for dc in range(2):
        for dx in range(4):
            if dx or dc:
                signal(barrier, device_in_line(0, 0, dx, dc))

    fetched = [
        pltpu.make_async_copy(source, target, insem.at[n])
        for n, (source, target) in enumerate([
            (value_hbm, value), (gate_hbm, gate), (taps_hbm, taps_in), (gain_hbm, gain_in),
            (ids_hbm, ids), (mix_hbm, mix), (ffn_gain_hbm, ffn_gain), (resid_hbm, resid),
            (ow_hbm, ow), (wg_hbm, wg), (wu_hbm, wu), (wd_hbm, wd),
        ])
    ]
    for copy in fetched:
        copy.start()
    for copy in fetched[:4]:
        copy.wait()

    def gated(g, carry):
        span = pl.ds(pl.multiple_of(g * 32, 32), 32)
        wide = value[span, :].astype(F32)
        glu[span, :] = (wide * sigmoid(gate[span, :].astype(F32))).astype(BF)
        return carry

    lax.fori_loop(0, 8, gated, 0)

    own_rows = pl.multiple_of(112 * tp, 16)
    inner = pl.multiple_of(16 * (1 - tp), 16)
    edge = pl.multiple_of(144 * tp, 16)
    inner_out = inner
    edge_out = pl.multiple_of(112 * tp, 16)

    def place(first, rows_of, taps_of, gain_of):
        for k in range(6):
            lanes = slice(k * 128, (k + 1) * 128)
            padded[first + k, pl.ds(inner, 144), :] = rows_of(lanes).astype(F32)
            taps[first + k, 0:31, :] = taps_of[:, lanes]
            taps[first + k, 31:32, :] = gain_of[lanes].reshape(1, 128)

    def convolve(block, start, count):
        total = jnp.zeros((count, 128), F32)
        for tap in range(31):
            total = total + padded[block, pl.ds(start + tap + 1, count), :] * taps[
                block, tap:tap + 1, :
            ]
        conv[block, pl.ds(start, count), :] = total

    def inner_blocks(first):
        def one(k, carry):
            convolve(first + k, inner_out, 56)
            convolve(first + k, inner_out + 56, 56)
            return carry

        lax.fori_loop(0, 6, one, 0)

    place(tp * 6, lambda lanes: glu[pl.ds(own_rows, 144), lanes], taps_in, gain_in)
    inner_blocks(tp * 6)
    expected = 13 + jnp.where(sp > 0, 1, 0) + jnp.where(sp < 63, 1, 0)
    pl.semaphore_wait(barrier, expected)

    to_next = pltpu.make_async_remote_copy(
        src_ref=glu.at[pl.ds(240, 16)], dst_ref=halo.at[tp], send_sem=hsend.at[0],
        recv_sem=hrecv.at[tp], device_id=(sp + 1, 0), device_id_type=MESH,
    )
    to_previous = pltpu.make_async_remote_copy(
        src_ref=glu.at[pl.ds(0, 16)], dst_ref=halo.at[tp], send_sem=hsend.at[1],
        recv_sem=hrecv.at[tp], device_id=(sp - 1, 1), device_id_type=MESH,
    )

    @pl.when(sp < 63)
    def _():
        to_next.start()

    @pl.when(sp > 0)
    def _():
        to_previous.start()

    for step in (2, 3, 1):
        signal(y_ready, device_in_line(0, step, 0, 0))
    peer_rows = pl.ds(pl.multiple_of(112 * (1 - tp), 16), 144)
    to_peer = [
        pltpu.make_async_remote_copy(
            src_ref=source, dst_ref=target, send_sem=gsend.at[n], recv_sem=grecv.at[n],
            device_id=(sp, 1 - tp), device_id_type=MESH,
        )
        for n, (source, target) in enumerate(
            [(glu.at[peer_rows], other), (taps_in, taps_other), (gain_in, gain_other)]
        )
    ]
    for copy in to_peer:
        copy.start()
    for copy in fetched[4:6]:
        copy.wait()

    slot = lax.broadcasted_iota(jnp.int32, (CAP * N, N), 0)
    i, r = slot // CAP, slot % CAP
    dz, dy, dx, dc = offsets(i)
    z, y, x = (sp // 16 + dz) % 4, ((sp // 4) % 4 + dy) % 4, (sp % 4 + dx) % 4
    expert = ((z * 4 + y) * 4 + x) * 2 + (tp + dc) % 2
    first = ids[0:1, :] == expert
    second = ids[1:2, :] == expert
    named = jnp.where(first | second, 1.0, 0.0)
    rows = lax.broadcasted_iota(jnp.int32, (N, N), 0)
    cols = lax.broadcasted_iota(jnp.int32, (N, N), 1)
    before = jnp.where(rows < cols, 1.0, 0.0).astype(BF)
    rank = jnp.dot(named.astype(BF), before, preferred_element_type=F32)
    chosen = jnp.where(rank == r.astype(F32), named, 0.0)
    gates[...] = chosen.astype(BF)
    weight = jnp.transpose(chosen * jnp.where(first, mix[0:1, :], mix[1:2, :]))
    high = weight.astype(BF)
    wt[0:N, :] = high
    wt[N:2 * N, :] = (weight - high.astype(F32)).astype(BF)

    for copy in to_peer:
        copy.wait_recv()
    place((1 - tp) * 6, lambda lanes: other[:, lanes], taps_other, gain_other)
    inner_blocks((1 - tp) * 6)
    pl.semaphore_wait(y_ready, 3)
    for step in (2, 3, 1):
        signal(z_ready, device_in_line(step, 0, 0, 0))

    def channel_norm(start, count):
        span = pl.ds(start, count)
        total = jnp.zeros((count, 128), F32)
        square = jnp.zeros((count, 128), F32)
        for k in range(12):
            part = conv[k, span, :]
            total = total + part
            square = square + part * part
        mean = jnp.sum(total, axis=1, keepdims=True) / 1536
        var = jnp.sum(square, axis=1, keepdims=True) / 1536 - mean * mean
        scale = lax.rsqrt(var + 1e-05)
        for k in range(12):
            part = (conv[k, span, :] - mean) * scale * taps[k, 31:32, :]
            mixed[span, k * 128:(k + 1) * 128] = (part * sigmoid(part)).astype(BF)

    channel_norm(inner_out, 112)

    @pl.when(has_halo)
    def _():
        for c in range(2):
            pltpu.make_async_remote_copy(
                src_ref=glu.at[pl.ds(0, 16)], dst_ref=halo.at[c], send_sem=hsend.at[0],
                recv_sem=hrecv.at[c], device_id=(sp, 1 - tp), device_id_type=MESH,
            ).wait_recv()
            for k in range(6):
                lanes = slice(k * 128, (k + 1) * 128)
                padded[c * 6 + k, pl.ds(edge, 16), :] = halo[c, :, lanes].astype(F32)

    @pl.when(jnp.logical_not(has_halo))
    def _():
        for k in range(12):
            padded[k, pl.ds(edge, 16), :] = jnp.zeros((16, 128), F32)

    def edges(k, carry):
        for part in range(4):
            convolve(4 * k + part, edge_out, 16)
        return carry

    lax.fori_loop(0, 3, edges, 0)
    channel_norm(edge_out, 16)
    for copy in fetched[6:9]:
        copy.wait()

    for j in range(2048 // TILE):
        col = slice(j * TILE, (j + 1) * TILE)
        part = jnp.dot(mixed[...], ow[:, col], preferred_element_type=F32)
        total = (resid[:, col].astype(F32) + part).astype(BF)
        stream[:, col] = total
        for group in range(512 // GATHER):
            part = jnp.dot(
                gates[group * GATHER:(group + 1) * GATHER, :], total, preferred_element_type=F32
            ).astype(BF)
            peers = slice(group * GATHER // CAP, (group + 1) * GATHER // CAP)
            sendbuf[peers, :, col] = part.reshape(GATHER // CAP, CAP, TILE)
    pl.semaphore_wait(z_ready, 3)

    def send_all(chunk, source, target, send, recv, sign, peers=PEERS):
        def one(i, carry):
            pltpu.make_async_remote_copy(
                src_ref=source.at[i], dst_ref=target.at[i], send_sem=send,
                recv_sem=recv.at[chunk], device_id=device_at(i, sign), device_id_type=MESH,
            ).start()
            return carry

        lax.fori_loop(max(1, chunk * peers), (chunk + 1) * peers, one, 0)

    def whole(chunk, source, target, send, recv, peers=PEERS):
        low = max(1, chunk * peers)
        span = pl.ds(low, (chunk + 1) * peers - low)
        return pltpu.make_async_remote_copy(
            src_ref=source.at[span], dst_ref=target.at[span], send_sem=send,
            recv_sem=recv.at[chunk], device_id=device_at(1, 1), device_id_type=MESH,
        )

    for chunk in range(CHUNKS):
        send_all(chunk, sendbuf, recvbuf, dsend, drecv, 1)
    recvbuf[0] = sendbuf[0]
    for copy in fetched[9:]:
        copy.wait()

    for chunk in range(CHUNKS):
        whole(chunk, sendbuf, recvbuf, dsend, drecv).wait_recv()
        peers = slice(chunk * PEERS, (chunk + 1) * PEERS)

        def normalise(g, carry):
            wide = recvbuf[pl.ds(chunk * PEERS + g * 4, 4)].reshape(16, 2048).astype(F32)
            mean = jnp.sum(wide * wide, axis=1, keepdims=True) / 2048
            normed = wide * lax.rsqrt(mean + 1e-06) * ffn_gain[...]
            xs[pl.ds(pl.multiple_of(g * 16, 16), 16), :] = normed.astype(BF)
            return carry

        lax.fori_loop(0, ROWS // 16, normalise, 0)

        def up(j, carry):
            col = pl.ds(pl.multiple_of(j * TILE, TILE), TILE)
            gated_part = jnp.dot(xs[...], wg[:, col], preferred_element_type=F32)
            up_part = jnp.dot(xs[...], wu[:, col], preferred_element_type=F32)
            hid[:, col] = (gated_part * sigmoid(gated_part) * up_part).astype(BF)
            return carry

        lax.fori_loop(0, 1024 // TILE, up, 0)

        def down(j, carry):
            col = pl.ds(pl.multiple_of(j * TILE, TILE), TILE)
            part = jnp.dot(hid[...], wd[:, col], preferred_element_type=F32).astype(BF)
            ysend[peers, :, col] = part.reshape(PEERS, CAP, TILE)
            return carry

        lax.fori_loop(0, 2048 // TILE, down, 0)
        if chunk == 0:
            yrecv[0] = ysend[0]
        for part in range(BACK // CHUNKS):
            send_all(chunk * BACK // CHUNKS + part, ysend, yrecv, rsend, rrecv, -1, N // BACK)

    for chunk in range(BACK):
        whole(chunk, ysend, yrecv, rsend, rrecv, N // BACK).wait_recv()
        peers = slice(chunk * N // BACK, (chunk + 1) * N // BACK)
        slots = slice(chunk * N // BACK * CAP, (chunk + 1) * N // BACK * CAP)

        for j in range(2048 // TILE):
            col = slice(j * TILE, (j + 1) * TILE)
            got = yrecv[peers, :, col].reshape(N // BACK * CAP, TILE)
            both = jnp.dot(wt[:, slots], got, preferred_element_type=F32)
            part = both[0:N] + both[N:2 * N]
            if chunk == 0:
                acc[:, col] = part + stream[:, col].astype(F32)
            elif chunk < BACK - 1:
                acc[:, col] = acc[:, col] + part
            else:
                out_ref[:, col] = acc[:, col] + part

    for chunk in range(CHUNKS):
        whole(chunk, sendbuf, recvbuf, dsend, drecv).wait_send()
    for chunk in range(BACK):
        whole(chunk, ysend, yrecv, rsend, rrecv, N // BACK).wait_send()
    for copy in to_peer:
        copy.wait_send()

    @pl.when(sp < 63)
    def _():
        to_next.wait_send()

    @pl.when(sp > 0)
    def _():
        to_previous.wait_send()


def per_device(
    resid,
    value_in,
    gate_in,
    conv_weight,
    norm_gain,
    out_weight,
    ffn_gain,
    expert_ids,
    expert_mix,
    w_gate,
    w_up,
    w_down,
):
    vmem = pl.BlockSpec(memory_space=pltpu.VMEM)
    hbm = pl.BlockSpec(memory_space=pltpu.HBM)
    slots = pltpu.VMEM((N, CAP, 2048), BF)
    dma = pltpu.SemaphoreType.DMA
    total = pl.pallas_call(
        layer_kernel,
        out_shape=pltpu.VMEM((N, 2048), F32),
        in_specs=[hbm] * 12,
        out_specs=vmem,
        scratch_shapes=[
            pltpu.VMEM((256, 768), BF),
            pltpu.VMEM((256, 768), BF),
            pltpu.VMEM((31, 768), F32),
            pltpu.VMEM((768,), F32),
            pltpu.VMEM((1, 2048), F32),
            pltpu.VMEM((2, N), jnp.int32),
            pltpu.VMEM((2, N), F32),
            pltpu.VMEM((N, 2048), BF),
            pltpu.VMEM((1536, 2048), BF),
            pltpu.VMEM((2048, 1024), BF),
            pltpu.VMEM((2048, 1024), BF),
            pltpu.VMEM((1024, 2048), BF),
            pltpu.VMEM((12, 32, 128), F32),
            pltpu.VMEM((31, 768), F32),
            pltpu.VMEM((768,), F32),
            pltpu.VMEM((256, 768), BF),
            pltpu.VMEM((144, 768), BF),
            pltpu.VMEM((2, 16, 768), BF),
            pltpu.VMEM((12, 160, 128), F32),
            pltpu.VMEM((12, 128, 128), F32),
            pltpu.VMEM((N, 1536), BF),
            pltpu.VMEM((N, 2048), BF),
            slots, slots, slots, slots,
            pltpu.VMEM((ROWS, 2048), BF),
            pltpu.VMEM((ROWS, 1024), BF),
            pltpu.VMEM((CAP * N, N), BF),
            pltpu.VMEM((2 * N, CAP * N), BF),
            pltpu.VMEM((N, 2048), F32),
            dma((12,)), dma((3,)), dma((3,)), dma((2,)), dma((2,)), dma, dma((CHUNKS,)), dma,
            dma((BACK,)), pltpu.SemaphoreType.REGULAR, pltpu.SemaphoreType.REGULAR,
        ],
        compiler_params=pltpu.CompilerParams(
            collective_id=0, has_side_effects=True, vmem_limit_bytes=60 * 2**20
        ),
        name="layer",
    )(
        resid, value_in, gate_in, conv_weight, norm_gain, out_weight,
        ffn_gain.reshape(1, 2048), expert_ids.T, expert_mix.T, w_gate[0], w_up[0], w_down[0],
    )
    return total.astype(BF)


def solution(mesh):
    return jax.shard_map(
        per_device,
        mesh=mesh,
        in_specs=(
            P(("sp", "tp"), None),
            P("sp", "tp"),
            P("sp", "tp"),
            P(None, "tp"),
            P("tp"),
            P(),
            P(),
            P(("sp", "tp"), None),
            P(("sp", "tp"), None),
            P(("sp", "tp"), None, None),
            P(("sp", "tp"), None, None),
            P(("sp", "tp"), None, None),
        ),
        out_specs=P(("sp", "tp"), None),
        check_vma=False,
    )
```

```python
import functools

import jax
import jax.numpy as jnp
from jax import lax
from jax.experimental import pallas as pl
from jax.experimental.pallas import tpu as pltpu
from jax.sharding import PartitionSpec as P

MESH = pl.DeviceIdType.MESH
BF = jnp.bfloat16
F32 = jnp.float32
CAP = 4
N = 128
TILE = 512
CHUNKS = 4
BACK = 4
PEERS = N // CHUNKS
ROWS = PEERS * CAP
GATHER = 256


def offsets(i):
    a, b, c = i % 4, (i // 4) % 4, (i // 16) % 4
    return a, (a + b) % 4, (a + b + c) % 4, (i // 64 + i) % 2


def sigmoid(v):
    return 0.5 * jnp.tanh(0.5 * v) + 0.5


def device_at(i, sign):
    sp, tp = lax.axis_index("sp"), lax.axis_index("tp")
    dz, dy, dx, dc = offsets(i)
    z, y, x = sp // 16, (sp // 4) % 4, sp % 4
    z, y, x = (z + 4 + sign * dz) % 4, (y + 4 + sign * dy) % 4, (x + 4 + sign * dx) % 4
    return (z * 4 + y) * 4 + x, (tp + dc) % 2


def device_in_line(dz, dy, dx, dc):
    sp, tp = lax.axis_index("sp"), lax.axis_index("tp")
    z, y, x = (sp // 16 + dz) % 4, ((sp // 4) % 4 + dy) % 4, (sp % 4 + dx) % 4
    return (z * 4 + y) * 4 + x, (tp + dc) % 2


def layer_kernel(
    resid_hbm, value_hbm, gate_hbm, taps_hbm, gain_hbm, ow_hbm, ffn_gain_hbm, ids_hbm, mix_hbm,
    wg_hbm, wu_hbm, wd_hbm,
    out_ref,
    value, gate, taps_in, gain_in, ffn_gain, ids, mix, resid, ow, wg, wu, wd,
    taps, taps_other, gain_other, glu, other, halo, padded, conv, mixed, stream,
    sendbuf, recvbuf, ysend, yrecv, xs, hid, gates, wt, acc,
    insem, gsend, grecv, hsend, hrecv, dsend, drecv, rsend, rrecv, y_ready, z_ready,
):
    sp, tp = lax.axis_index("sp"), lax.axis_index("tp")
    barrier = pltpu.get_barrier_semaphore()

    def signal(semaphore, device):
        pl.semaphore_signal(semaphore, inc=1, device_id=device, device_id_type=MESH)

    halo_from = jnp.where(tp == 0, sp - 1, sp + 1)
    has_halo = (halo_from >= 0) & (halo_from < 64)

    @pl.when(has_halo)
    def _():
        signal(barrier, (halo_from, 0))
        signal(barrier, (halo_from, 1))

    for step in (2, 3, 1):
        signal(barrier, device_in_line(0, step, 0, 0))
        signal(barrier, device_in_line(step, 0, 0, 0))
    for dc in range(2):
        for dx in range(4):
            if dx or dc:
                signal(barrier, device_in_line(0, 0, dx, dc))

    fetched = [
        pltpu.make_async_copy(source, target, insem.at[n])
        for n, (source, target) in enumerate([
            (value_hbm, value), (gate_hbm, gate), (taps_hbm, taps_in), (gain_hbm, gain_in),
            (ids_hbm, ids), (mix_hbm, mix), (ffn_gain_hbm, ffn_gain), (resid_hbm, resid),
            (ow_hbm, ow), (wg_hbm, wg), (wu_hbm, wu), (wd_hbm, wd),
        ])
    ]
    for copy in fetched[:9]:
        copy.start()
    slot = lax.broadcasted_iota(jnp.int32, (CAP * N, N), 0)
    i, r = slot // CAP, slot % CAP
    dz, dy, dx, dc = offsets(i)
    z, y, x = (sp // 16 + dz) % 4, ((sp // 4) % 4 + dy) % 4, (sp % 4 + dx) % 4
    expert = ((z * 4 + y) * 4 + x) * 2 + (tp + dc) % 2
    rows = lax.broadcasted_iota(jnp.int32, (N, N), 0)
    cols = lax.broadcasted_iota(jnp.int32, (N, N), 1)
    before = jnp.where(rows < cols, 1.0, 0.0).astype(BF)
    rank_of_slot = r.astype(F32)
    for copy in fetched[:4]:
        copy.wait()

    def gated(g, carry):
        span = pl.ds(pl.multiple_of(g * 32, 32), 32)
        wide = value[span, :].astype(F32)
        glu[span, :] = (wide * sigmoid(gate[span, :].astype(F32))).astype(BF)
        return carry

    lax.fori_loop(0, 8, gated, 0)

    own_rows = pl.multiple_of(112 * tp, 16)
    inner = pl.multiple_of(16 * (1 - tp), 16)
    edge = pl.multiple_of(144 * tp, 16)
    inner_out = inner
    edge_out = pl.multiple_of(112 * tp, 16)

    def place(first, rows_of, taps_of, gain_of):
        for k in range(6):
            lanes = slice(k * 128, (k + 1) * 128)
            padded[first + k, pl.ds(inner, 144), :] = rows_of(lanes).astype(F32)
            taps[first + k, 0:31, :] = taps_of[:, lanes]
            taps[first + k, 31:32, :] = gain_of[lanes].reshape(1, 128)

    def convolve(block, start, count):
        total = jnp.zeros((count, 128), F32)
        for tap in range(31):
            total = total + padded[block, pl.ds(start + tap + 1, count), :] * taps[
                block, tap:tap + 1, :
            ]
        conv[block, pl.ds(start, count), :] = total

    def inner_blocks(first):
        def one(k, carry):
            convolve(first + k, inner_out, 56)
            convolve(first + k, inner_out + 56, 56)
            return carry

        lax.fori_loop(0, 6, one, 0)

    expected = 13 + jnp.where(sp > 0, 1, 0) + jnp.where(sp < 63, 1, 0)
    pl.semaphore_wait(barrier, expected)

    to_next = pltpu.make_async_remote_copy(
        src_ref=glu.at[pl.ds(240, 16)], dst_ref=halo.at[tp], send_sem=hsend.at[0],
        recv_sem=hrecv.at[tp], device_id=(sp + 1, 0), device_id_type=MESH,
    )
    to_previous = pltpu.make_async_remote_copy(
        src_ref=glu.at[pl.ds(0, 16)], dst_ref=halo.at[tp], send_sem=hsend.at[1],
        recv_sem=hrecv.at[tp], device_id=(sp - 1, 1), device_id_type=MESH,
    )

    @pl.when(sp < 63)
    def _():
        to_next.start()

    @pl.when(sp > 0)
    def _():
        to_previous.start()

    for step in (2, 3, 1):
        signal(y_ready, device_in_line(0, step, 0, 0))
    peer_rows = pl.ds(pl.multiple_of(112 * (1 - tp), 16), 144)
    to_peer = [
        pltpu.make_async_remote_copy(
            src_ref=source, dst_ref=target, send_sem=gsend.at[n], recv_sem=grecv.at[n],
            device_id=(sp, 1 - tp), device_id_type=MESH,
        )
        for n, (source, target) in enumerate(
            [(glu.at[peer_rows], other), (taps_in, taps_other), (gain_in, gain_other)]
        )
    ]
    for copy in to_peer:
        copy.start()
    place(tp * 6, lambda lanes: glu[pl.ds(own_rows, 144), lanes], taps_in, gain_in)
    inner_blocks(tp * 6)
    for copy in fetched[4:6]:
        copy.wait()

    first = ids[0:1, :] == expert
    second = ids[1:2, :] == expert
    named = jnp.where(first | second, 1.0, 0.0)
    rank = jnp.dot(named.astype(BF), before, preferred_element_type=F32)
    chosen = jnp.where(rank == rank_of_slot, named, 0.0)
    gates[...] = chosen.astype(BF)
    weight = jnp.transpose(chosen * jnp.where(first, mix[0:1, :], mix[1:2, :]))
    high = weight.astype(BF)
    wt[0:N, :] = high
    wt[N:2 * N, :] = (weight - high.astype(F32)).astype(BF)

    pl.semaphore_wait(y_ready, 3)
    for step in (2, 3, 1):
        signal(z_ready, device_in_line(step, 0, 0, 0))
    for copy in to_peer:
        copy.wait_recv()
    place((1 - tp) * 6, lambda lanes: other[:, lanes], taps_other, gain_other)
    inner_blocks((1 - tp) * 6)

    def channel_norm(start, count):
        span = pl.ds(start, count)
        total = jnp.zeros((count, 128), F32)
        square = jnp.zeros((count, 128), F32)
        for k in range(12):
            part = conv[k, span, :]
            total = total + part
            square = square + part * part
        mean = jnp.sum(total, axis=1, keepdims=True) / 1536
        var = jnp.sum(square, axis=1, keepdims=True) / 1536 - mean * mean
        scale = lax.rsqrt(var + 1e-05)
        for k in range(12):
            part = (conv[k, span, :] - mean) * scale * taps[k, 31:32, :]
            mixed[span, k * 128:(k + 1) * 128] = (part * sigmoid(part)).astype(BF)

    channel_norm(inner_out, 112)

    @pl.when(has_halo)
    def _():
        for c in range(2):
            pltpu.make_async_remote_copy(
                src_ref=glu.at[pl.ds(0, 16)], dst_ref=halo.at[c], send_sem=hsend.at[0],
                recv_sem=hrecv.at[c], device_id=(sp, 1 - tp), device_id_type=MESH,
            ).wait_recv()
            for k in range(6):
                lanes = slice(k * 128, (k + 1) * 128)
                padded[c * 6 + k, pl.ds(edge, 16), :] = halo[c, :, lanes].astype(F32)

    @pl.when(jnp.logical_not(has_halo))
    def _():
        for k in range(12):
            padded[k, pl.ds(edge, 16), :] = jnp.zeros((16, 128), F32)

    def edges(k, carry):
        for part in range(4):
            convolve(4 * k + part, edge_out, 16)
        return carry

    lax.fori_loop(0, 3, edges, 0)
    channel_norm(edge_out, 16)
    for copy in fetched[6:9]:
        copy.wait()

    for j in range(2048 // TILE):
        col = slice(j * TILE, (j + 1) * TILE)
        part = jnp.dot(mixed[...], ow[:, col], preferred_element_type=F32)
        total = (resid[:, col].astype(F32) + part).astype(BF)
        stream[:, col] = total
        for group in range(512 // GATHER):
            part = jnp.dot(
                gates[group * GATHER:(group + 1) * GATHER, :], total, preferred_element_type=F32
            ).astype(BF)
            peers = slice(group * GATHER // CAP, (group + 1) * GATHER // CAP)
            sendbuf[peers, :, col] = part.reshape(GATHER // CAP, CAP, TILE)
    pl.semaphore_wait(z_ready, 3)

    def send_all(chunk, source, target, send, recv, sign, peers=PEERS):
        def one(i, carry):
            pltpu.make_async_remote_copy(
                src_ref=source.at[i], dst_ref=target.at[i], send_sem=send,
                recv_sem=recv.at[chunk], device_id=device_at(i, sign), device_id_type=MESH,
            ).start()
            return carry

        lax.fori_loop(max(1, chunk * peers), (chunk + 1) * peers, one, 0)

    def whole(chunk, source, target, send, recv, peers=PEERS):
        low = max(1, chunk * peers)
        span = pl.ds(low, (chunk + 1) * peers - low)
        return pltpu.make_async_remote_copy(
            src_ref=source.at[span], dst_ref=target.at[span], send_sem=send,
            recv_sem=recv.at[chunk], device_id=device_at(1, 1), device_id_type=MESH,
        )

    for chunk in range(CHUNKS):
        send_all(chunk, sendbuf, recvbuf, dsend, drecv, 1)
    for copy in fetched[9:]:
        copy.start()
    recvbuf[0] = sendbuf[0]
    for copy in fetched[9:]:
        copy.wait()

    for chunk in range(CHUNKS):
        whole(chunk, sendbuf, recvbuf, dsend, drecv).wait_recv()
        peers = slice(chunk * PEERS, (chunk + 1) * PEERS)

        def normalise(g, carry):
            wide = recvbuf[pl.ds(chunk * PEERS + g * 4, 4)].reshape(16, 2048).astype(F32)
            mean = jnp.sum(wide * wide, axis=1, keepdims=True) / 2048
            normed = wide * lax.rsqrt(mean + 1e-06) * ffn_gain[...]
            xs[pl.ds(pl.multiple_of(g * 16, 16), 16), :] = normed.astype(BF)
            return carry

        lax.fori_loop(0, ROWS // 16, normalise, 0)

        def up(j, carry):
            col = pl.ds(pl.multiple_of(j * TILE, TILE), TILE)
            gated_part = jnp.dot(xs[...], wg[:, col], preferred_element_type=F32)
            up_part = jnp.dot(xs[...], wu[:, col], preferred_element_type=F32)
            hid[:, col] = (gated_part * sigmoid(gated_part) * up_part).astype(BF)
            return carry

        lax.fori_loop(0, 1024 // TILE, up, 0)

        def down(j, carry):
            col = pl.ds(pl.multiple_of(j * TILE, TILE), TILE)
            part = jnp.dot(hid[...], wd[:, col], preferred_element_type=F32).astype(BF)
            ysend[peers, :, col] = part.reshape(PEERS, CAP, TILE)
            return carry

        lax.fori_loop(0, 2048 // TILE, down, 0)
        if chunk == 0:
            yrecv[0] = ysend[0]
        for part in range(BACK // CHUNKS):
            send_all(chunk * BACK // CHUNKS + part, ysend, yrecv, rsend, rrecv, -1, N // BACK)

    for chunk in range(BACK):
        whole(chunk, ysend, yrecv, rsend, rrecv, N // BACK).wait_recv()
        peers = slice(chunk * N // BACK, (chunk + 1) * N // BACK)
        slots = slice(chunk * N // BACK * CAP, (chunk + 1) * N // BACK * CAP)

        for j in range(2048 // TILE):
            col = slice(j * TILE, (j + 1) * TILE)
            got = yrecv[peers, :, col].reshape(N // BACK * CAP, TILE)
            both = jnp.dot(wt[:, slots], got, preferred_element_type=F32)
            part = both[0:N] + both[N:2 * N]
            if chunk == 0:
                acc[:, col] = part + stream[:, col].astype(F32)
            elif chunk < BACK - 1:
                acc[:, col] = acc[:, col] + part
            else:
                out_ref[:, col] = acc[:, col] + part

    for chunk in range(CHUNKS):
        whole(chunk, sendbuf, recvbuf, dsend, drecv).wait_send()
    for chunk in range(BACK):
        whole(chunk, ysend, yrecv, rsend, rrecv, N // BACK).wait_send()
    for copy in to_peer:
        copy.wait_send()

    @pl.when(sp < 63)
    def _():
        to_next.wait_send()

    @pl.when(sp > 0)
    def _():
        to_previous.wait_send()


def per_device(
    resid,
    value_in,
    gate_in,
    conv_weight,
    norm_gain,
    out_weight,
    ffn_gain,
    expert_ids,
    expert_mix,
    w_gate,
    w_up,
    w_down,
):
    vmem = pl.BlockSpec(memory_space=pltpu.VMEM)
    hbm = pl.BlockSpec(memory_space=pltpu.HBM)
    slots = pltpu.VMEM((N, CAP, 2048), BF)
    dma = pltpu.SemaphoreType.DMA
    total = pl.pallas_call(
        layer_kernel,
        out_shape=pltpu.VMEM((N, 2048), F32),
        in_specs=[hbm] * 12,
        out_specs=vmem,
        scratch_shapes=[
            pltpu.VMEM((256, 768), BF),
            pltpu.VMEM((256, 768), BF),
            pltpu.VMEM((31, 768), F32),
            pltpu.VMEM((768,), F32),
            pltpu.VMEM((1, 2048), F32),
            pltpu.VMEM((2, N), jnp.int32),
            pltpu.VMEM((2, N), F32),
            pltpu.VMEM((N, 2048), BF),
            pltpu.VMEM((1536, 2048), BF),
            pltpu.VMEM((2048, 1024), BF),
            pltpu.VMEM((2048, 1024), BF),
            pltpu.VMEM((1024, 2048), BF),
            pltpu.VMEM((12, 32, 128), F32),
            pltpu.VMEM((31, 768), F32),
            pltpu.VMEM((768,), F32),
            pltpu.VMEM((256, 768), BF),
            pltpu.VMEM((144, 768), BF),
            pltpu.VMEM((2, 16, 768), BF),
            pltpu.VMEM((12, 160, 128), F32),
            pltpu.VMEM((12, 128, 128), F32),
            pltpu.VMEM((N, 1536), BF),
            pltpu.VMEM((N, 2048), BF),
            slots, slots, slots, slots,
            pltpu.VMEM((ROWS, 2048), BF),
            pltpu.VMEM((ROWS, 1024), BF),
            pltpu.VMEM((CAP * N, N), BF),
            pltpu.VMEM((2 * N, CAP * N), BF),
            pltpu.VMEM((N, 2048), F32),
            dma((12,)), dma((3,)), dma((3,)), dma((2,)), dma((2,)), dma, dma((CHUNKS,)), dma,
            dma((BACK,)), pltpu.SemaphoreType.REGULAR, pltpu.SemaphoreType.REGULAR,
        ],
        compiler_params=pltpu.CompilerParams(
            collective_id=0, has_side_effects=True, vmem_limit_bytes=60 * 2**20
        ),
        name="layer",
    )(
        resid, value_in, gate_in, conv_weight, norm_gain, out_weight,
        ffn_gain.reshape(1, 2048), expert_ids.T, expert_mix.T, w_gate[0], w_up[0], w_down[0],
    )
    return total.astype(BF)


def solution(mesh):
    return jax.shard_map(
        per_device,
        mesh=mesh,
        in_specs=(
            P(("sp", "tp"), None),
            P("sp", "tp"),
            P("sp", "tp"),
            P(None, "tp"),
            P("tp"),
            P(),
            P(),
            P(("sp", "tp"), None),
            P(("sp", "tp"), None),
            P(("sp", "tp"), None, None),
            P(("sp", "tp"), None, None),
            P(("sp", "tp"), None, None),
        ),
        out_specs=P(("sp", "tp"), None),
        check_vma=False,
    )
```

```python
import functools

import jax
import jax.numpy as jnp
from jax import lax
from jax.experimental import pallas as pl
from jax.experimental.pallas import tpu as pltpu
from jax.sharding import PartitionSpec as P

MESH = pl.DeviceIdType.MESH
BF = jnp.bfloat16
F32 = jnp.float32
CAP = 4
N = 128
TILE = 512
CHUNKS = 4
BACK = 4
PEERS = N // CHUNKS
ROWS = PEERS * CAP
GATHER = 256


def offsets(i):
    a, b, c = i % 4, (i // 4) % 4, (i // 16) % 4
    return a, (a + b) % 4, (a + b + c) % 4, (i // 64 + i) % 2


def sigmoid(v):
    return 0.5 * jnp.tanh(0.5 * v) + 0.5


def device_at(i, sign):
    sp, tp = lax.axis_index("sp"), lax.axis_index("tp")
    dz, dy, dx, dc = offsets(i)
    z, y, x = sp // 16, (sp // 4) % 4, sp % 4
    z, y, x = (z + 4 + sign * dz) % 4, (y + 4 + sign * dy) % 4, (x + 4 + sign * dx) % 4
    return (z * 4 + y) * 4 + x, (tp + dc) % 2


def device_in_line(dz, dy, dx, dc):
    sp, tp = lax.axis_index("sp"), lax.axis_index("tp")
    z, y, x = (sp // 16 + dz) % 4, ((sp // 4) % 4 + dy) % 4, (sp % 4 + dx) % 4
    return (z * 4 + y) * 4 + x, (tp + dc) % 2


def layer_kernel(
    resid_hbm, value_hbm, gate_hbm, taps_hbm, gain_hbm, ow_hbm, ffn_gain_hbm, ids_hbm, mix_hbm,
    wg_hbm, wu_hbm, wd_hbm,
    out_ref,
    value, gate, taps_in, gain_in, ffn_gain, ids, mix, resid, ow, wg, wu, wd,
    taps, taps_other, gain_other, glu, other, halo, padded, conv, mixed, stream,
    sendbuf, recvbuf, ysend, yrecv, xs, hid, gates, wt, acc,
    insem, gsend, grecv, hsend, hrecv, dsend, drecv, rsend, rrecv, y_ready, z_ready,
):
    sp, tp = lax.axis_index("sp"), lax.axis_index("tp")
    barrier = pltpu.get_barrier_semaphore()

    def signal(semaphore, device):
        pl.semaphore_signal(semaphore, inc=1, device_id=device, device_id_type=MESH)

    halo_from = jnp.where(tp == 0, sp - 1, sp + 1)
    has_halo = (halo_from >= 0) & (halo_from < 64)

    @pl.when(has_halo)
    def _():
        signal(barrier, (halo_from, 0))
        signal(barrier, (halo_from, 1))

    for step in (2, 3, 1):
        signal(barrier, device_in_line(0, step, 0, 0))
        signal(barrier, device_in_line(step, 0, 0, 0))
    for dc in range(2):
        for dx in range(4):
            if dx or dc:
                signal(barrier, device_in_line(0, 0, dx, dc))

    fetched = [
        pltpu.make_async_copy(source, target, insem.at[n])
        for n, (source, target) in enumerate([
            (value_hbm, value), (gate_hbm, gate), (taps_hbm, taps_in), (gain_hbm, gain_in),
            (ids_hbm, ids), (mix_hbm, mix), (ffn_gain_hbm, ffn_gain), (resid_hbm, resid),
            (ow_hbm, ow), (wg_hbm, wg), (wu_hbm, wu), (wd_hbm, wd),
        ])
    ]
    for copy in fetched[:9]:
        copy.start()
    slot = lax.broadcasted_iota(jnp.int32, (CAP * N, N), 0)
    i, r = slot // CAP, slot % CAP
    dz, dy, dx, dc = offsets(i)
    z, y, x = (sp // 16 + dz) % 4, ((sp // 4) % 4 + dy) % 4, (sp % 4 + dx) % 4
    expert = ((z * 4 + y) * 4 + x) * 2 + (tp + dc) % 2
    rows = lax.broadcasted_iota(jnp.int32, (N, N), 0)
    cols = lax.broadcasted_iota(jnp.int32, (N, N), 1)
    before = jnp.where(rows < cols, 1.0, 0.0).astype(BF)
    rank_of_slot = r.astype(F32)
    for copy in fetched[:4]:
        copy.wait()

    def gated(g, carry):
        span = pl.ds(pl.multiple_of(g * 32, 32), 32)
        wide = value[span, :].astype(F32)
        glu[span, :] = (wide * sigmoid(gate[span, :].astype(F32))).astype(BF)
        return carry

    lax.fori_loop(0, 8, gated, 0)

    own_rows = pl.multiple_of(112 * tp, 16)
    inner = pl.multiple_of(16 * (1 - tp), 16)
    edge = pl.multiple_of(144 * tp, 16)
    inner_out = inner
    edge_out = pl.multiple_of(112 * tp, 16)

    def place(first, rows_of, taps_of, gain_of):
        for k in range(6):
            lanes = slice(k * 128, (k + 1) * 128)
            padded[first + k, pl.ds(inner, 144), :] = rows_of(lanes).astype(F32)
            taps[first + k, 0:31, :] = taps_of[:, lanes]
            taps[first + k, 31:32, :] = gain_of[lanes].reshape(1, 128)

    def convolve(block, start, count):
        total = jnp.zeros((count, 128), F32)
        for tap in range(31):
            total = total + padded[block, pl.ds(start + tap + 1, count), :] * taps[
                block, tap:tap + 1, :
            ]
        conv[block, pl.ds(start, count), :] = total

    def inner_blocks(first):
        def one(k, carry):
            convolve(first + k, inner_out, 56)
            convolve(first + k, inner_out + 56, 56)
            return carry

        lax.fori_loop(0, 6, one, 0)

    expected = 13 + jnp.where(sp > 0, 1, 0) + jnp.where(sp < 63, 1, 0)
    pl.semaphore_wait(barrier, expected)

    to_next = pltpu.make_async_remote_copy(
        src_ref=glu.at[pl.ds(240, 16)], dst_ref=halo.at[tp], send_sem=hsend.at[0],
        recv_sem=hrecv.at[tp], device_id=(sp + 1, 0), device_id_type=MESH,
    )
    to_previous = pltpu.make_async_remote_copy(
        src_ref=glu.at[pl.ds(0, 16)], dst_ref=halo.at[tp], send_sem=hsend.at[1],
        recv_sem=hrecv.at[tp], device_id=(sp - 1, 1), device_id_type=MESH,
    )

    @pl.when(sp < 63)
    def _():
        to_next.start()

    @pl.when(sp > 0)
    def _():
        to_previous.start()

    for step in (2, 3, 1):
        signal(z_ready, device_in_line(step, 0, 0, 0))
    peer_rows = pl.ds(pl.multiple_of(112 * (1 - tp), 16), 144)
    to_peer = [
        pltpu.make_async_remote_copy(
            src_ref=source, dst_ref=target, send_sem=gsend.at[n], recv_sem=grecv.at[n],
            device_id=(sp, 1 - tp), device_id_type=MESH,
        )
        for n, (source, target) in enumerate(
            [(glu.at[peer_rows], other), (taps_in, taps_other), (gain_in, gain_other)]
        )
    ]
    for copy in to_peer:
        copy.start()
    place(tp * 6, lambda lanes: glu[pl.ds(own_rows, 144), lanes], taps_in, gain_in)
    inner_blocks(tp * 6)
    for copy in fetched[4:6]:
        copy.wait()

    first = ids[0:1, :] == expert
    second = ids[1:2, :] == expert
    named = jnp.where(first | second, 1.0, 0.0)
    rank = jnp.dot(named.astype(BF), before, preferred_element_type=F32)
    chosen = jnp.where(rank == rank_of_slot, named, 0.0)
    gates[...] = chosen.astype(BF)
    weight = jnp.transpose(chosen * jnp.where(first, mix[0:1, :], mix[1:2, :]))
    high = weight.astype(BF)
    wt[0:N, :] = high
    wt[N:2 * N, :] = (weight - high.astype(F32)).astype(BF)

    pl.semaphore_wait(z_ready, 3)
    for step in (2, 3, 1):
        signal(y_ready, device_in_line(0, step, 0, 0))
    for copy in to_peer:
        copy.wait_recv()
    place((1 - tp) * 6, lambda lanes: other[:, lanes], taps_other, gain_other)
    inner_blocks((1 - tp) * 6)

    def channel_norm(start, count):
        span = pl.ds(start, count)
        total = jnp.zeros((count, 128), F32)
        square = jnp.zeros((count, 128), F32)
        for k in range(12):
            part = conv[k, span, :]
            total = total + part
            square = square + part * part
        mean = jnp.sum(total, axis=1, keepdims=True) / 1536
        var = jnp.sum(square, axis=1, keepdims=True) / 1536 - mean * mean
        scale = lax.rsqrt(var + 1e-05)
        for k in range(12):
            part = (conv[k, span, :] - mean) * scale * taps[k, 31:32, :]
            mixed[span, k * 128:(k + 1) * 128] = (part * sigmoid(part)).astype(BF)

    channel_norm(inner_out, 112)

    @pl.when(has_halo)
    def _():
        for c in range(2):
            pltpu.make_async_remote_copy(
                src_ref=glu.at[pl.ds(0, 16)], dst_ref=halo.at[c], send_sem=hsend.at[0],
                recv_sem=hrecv.at[c], device_id=(sp, 1 - tp), device_id_type=MESH,
            ).wait_recv()
            for k in range(6):
                lanes = slice(k * 128, (k + 1) * 128)
                padded[c * 6 + k, pl.ds(edge, 16), :] = halo[c, :, lanes].astype(F32)

    @pl.when(jnp.logical_not(has_halo))
    def _():
        for k in range(12):
            padded[k, pl.ds(edge, 16), :] = jnp.zeros((16, 128), F32)

    def edges(k, carry):
        for part in range(4):
            convolve(4 * k + part, edge_out, 16)
        return carry

    lax.fori_loop(0, 3, edges, 0)
    channel_norm(edge_out, 16)
    for copy in fetched[6:9]:
        copy.wait()

    for j in range(2048 // TILE):
        col = slice(j * TILE, (j + 1) * TILE)
        part = jnp.dot(mixed[...], ow[:, col], preferred_element_type=F32)
        total = (resid[:, col].astype(F32) + part).astype(BF)
        stream[:, col] = total
        for group in range(512 // GATHER):
            part = jnp.dot(
                gates[group * GATHER:(group + 1) * GATHER, :], total, preferred_element_type=F32
            ).astype(BF)
            peers = slice(group * GATHER // CAP, (group + 1) * GATHER // CAP)
            sendbuf[peers, :, col] = part.reshape(GATHER // CAP, CAP, TILE)
    pl.semaphore_wait(y_ready, 3)

    def send_all(chunk, source, target, send, recv, sign, peers=PEERS):
        def one(i, carry):
            pltpu.make_async_remote_copy(
                src_ref=source.at[i], dst_ref=target.at[i], send_sem=send,
                recv_sem=recv.at[chunk], device_id=device_at(i, sign), device_id_type=MESH,
            ).start()
            return carry

        lax.fori_loop(max(1, chunk * peers), (chunk + 1) * peers, one, 0)

    def whole(chunk, source, target, send, recv, peers=PEERS):
        low = max(1, chunk * peers)
        span = pl.ds(low, (chunk + 1) * peers - low)
        return pltpu.make_async_remote_copy(
            src_ref=source.at[span], dst_ref=target.at[span], send_sem=send,
            recv_sem=recv.at[chunk], device_id=device_at(1, 1), device_id_type=MESH,
        )

    for chunk in range(CHUNKS):
        send_all(chunk, sendbuf, recvbuf, dsend, drecv, 1)
    for copy in fetched[9:]:
        copy.start()
    recvbuf[0] = sendbuf[0]
    for copy in fetched[9:]:
        copy.wait()

    for chunk in range(CHUNKS):
        whole(chunk, sendbuf, recvbuf, dsend, drecv).wait_recv()
        peers = slice(chunk * PEERS, (chunk + 1) * PEERS)

        def normalise(g, carry):
            wide = recvbuf[pl.ds(chunk * PEERS + g * 4, 4)].reshape(16, 2048).astype(F32)
            mean = jnp.sum(wide * wide, axis=1, keepdims=True) / 2048
            normed = wide * lax.rsqrt(mean + 1e-06) * ffn_gain[...]
            xs[pl.ds(pl.multiple_of(g * 16, 16), 16), :] = normed.astype(BF)
            return carry

        lax.fori_loop(0, ROWS // 16, normalise, 0)

        def up(j, carry):
            col = pl.ds(pl.multiple_of(j * TILE, TILE), TILE)
            gated_part = jnp.dot(xs[...], wg[:, col], preferred_element_type=F32)
            up_part = jnp.dot(xs[...], wu[:, col], preferred_element_type=F32)
            hid[:, col] = (gated_part * sigmoid(gated_part) * up_part).astype(BF)
            return carry

        lax.fori_loop(0, 1024 // TILE, up, 0)

        def down(j, carry):
            col = pl.ds(pl.multiple_of(j * TILE, TILE), TILE)
            part = jnp.dot(hid[...], wd[:, col], preferred_element_type=F32).astype(BF)
            ysend[peers, :, col] = part.reshape(PEERS, CAP, TILE)
            return carry

        lax.fori_loop(0, 2048 // TILE, down, 0)
        if chunk == 0:
            yrecv[0] = ysend[0]
        for part in range(BACK // CHUNKS):
            send_all(chunk * BACK // CHUNKS + part, ysend, yrecv, rsend, rrecv, -1, N // BACK)

    for chunk in range(BACK):
        whole(chunk, ysend, yrecv, rsend, rrecv, N // BACK).wait_recv()
        peers = slice(chunk * N // BACK, (chunk + 1) * N // BACK)
        slots = slice(chunk * N // BACK * CAP, (chunk + 1) * N // BACK * CAP)

        for j in range(2048 // TILE):
            col = slice(j * TILE, (j + 1) * TILE)
            got = yrecv[peers, :, col].reshape(N // BACK * CAP, TILE)
            both = jnp.dot(wt[:, slots], got, preferred_element_type=F32)
            part = both[0:N] + both[N:2 * N]
            if chunk == 0:
                acc[:, col] = part + stream[:, col].astype(F32)
            elif chunk < BACK - 1:
                acc[:, col] = acc[:, col] + part
            else:
                out_ref[:, col] = acc[:, col] + part

    for chunk in range(CHUNKS):
        whole(chunk, sendbuf, recvbuf, dsend, drecv).wait_send()
    for chunk in range(BACK):
        whole(chunk, ysend, yrecv, rsend, rrecv, N // BACK).wait_send()
    for copy in to_peer:
        copy.wait_send()

    @pl.when(sp < 63)
    def _():
        to_next.wait_send()

    @pl.when(sp > 0)
    def _():
        to_previous.wait_send()


def per_device(
    resid,
    value_in,
    gate_in,
    conv_weight,
    norm_gain,
    out_weight,
    ffn_gain,
    expert_ids,
    expert_mix,
    w_gate,
    w_up,
    w_down,
):
    vmem = pl.BlockSpec(memory_space=pltpu.VMEM)
    hbm = pl.BlockSpec(memory_space=pltpu.HBM)
    slots = pltpu.VMEM((N, CAP, 2048), BF)
    dma = pltpu.SemaphoreType.DMA
    total = pl.pallas_call(
        layer_kernel,
        out_shape=pltpu.VMEM((N, 2048), F32),
        in_specs=[hbm] * 12,
        out_specs=vmem,
        scratch_shapes=[
            pltpu.VMEM((256, 768), BF),
            pltpu.VMEM((256, 768), BF),
            pltpu.VMEM((31, 768), F32),
            pltpu.VMEM((768,), F32),
            pltpu.VMEM((1, 2048), F32),
            pltpu.VMEM((2, N), jnp.int32),
            pltpu.VMEM((2, N), F32),
            pltpu.VMEM((N, 2048), BF),
            pltpu.VMEM((1536, 2048), BF),
            pltpu.VMEM((2048, 1024), BF),
            pltpu.VMEM((2048, 1024), BF),
            pltpu.VMEM((1024, 2048), BF),
            pltpu.VMEM((12, 32, 128), F32),
            pltpu.VMEM((31, 768), F32),
            pltpu.VMEM((768,), F32),
            pltpu.VMEM((256, 768), BF),
            pltpu.VMEM((144, 768), BF),
            pltpu.VMEM((2, 16, 768), BF),
            pltpu.VMEM((12, 160, 128), F32),
            pltpu.VMEM((12, 128, 128), F32),
            pltpu.VMEM((N, 1536), BF),
            pltpu.VMEM((N, 2048), BF),
            slots, slots, slots, slots,
            pltpu.VMEM((ROWS, 2048), BF),
            pltpu.VMEM((ROWS, 1024), BF),
            pltpu.VMEM((CAP * N, N), BF),
            pltpu.VMEM((2 * N, CAP * N), BF),
            pltpu.VMEM((N, 2048), F32),
            dma((12,)), dma((3,)), dma((3,)), dma((2,)), dma((2,)), dma, dma((CHUNKS,)), dma,
            dma((BACK,)), pltpu.SemaphoreType.REGULAR, pltpu.SemaphoreType.REGULAR,
        ],
        compiler_params=pltpu.CompilerParams(
            collective_id=0, has_side_effects=True, vmem_limit_bytes=60 * 2**20
        ),
        name="layer",
    )(
        resid, value_in, gate_in, conv_weight, norm_gain, out_weight,
        ffn_gain.reshape(1, 2048), expert_ids.T, expert_mix.T, w_gate[0], w_up[0], w_down[0],
    )
    return total.astype(BF)


def solution(mesh):
    return jax.shard_map(
        per_device,
        mesh=mesh,
        in_specs=(
            P(("sp", "tp"), None),
            P("sp", "tp"),
            P("sp", "tp"),
            P(None, "tp"),
            P("tp"),
            P(),
            P(),
            P(("sp", "tp"), None),
            P(("sp", "tp"), None),
            P(("sp", "tp"), None, None),
            P(("sp", "tp"), None, None),
            P(("sp", "tp"), None, None),
        ),
        out_specs=P(("sp", "tp"), None),
        check_vma=False,
    )
```
